32 devices in a mesh: sp: 4 (over z), fs: 4 (over y, core), tp: 2 (over x).
Axes of the slice: x: 2, y: 2, z: 4, core: 2. Of those that a mesh axis runs over, the one named last changes fastest.
Arguments:
- tokens: bfloat16 [4, 768, 2048], P('fs', 'sp'), may hold values from -6 to 6
- decay_pace: float32 [4, 768], P('fs', 'sp'), may hold values from 0.5 to 2, as said below
- start_state: float32 [4, 16, 64, 64], P('fs', 'tp'), may hold values from -80 to 80
- norm_gain: float32 [2048], replicated, may hold values from 0.1 to 1.9
- conv_value: bfloat16 [2048, 512], P(('sp', 'fs'), 'tp'), may hold values from -0.125 to 0.125
- conv_admit: bfloat16 [2048, 512], P(('sp', 'fs'), 'tp'), may hold values from -0.125 to 0.125
- conv_gate: bfloat16 [2048, 512], P(('sp', 'fs'), 'tp'), may hold values from -0.125 to 0.125
- state_query: bfloat16 [2048, 1024], P(('sp', 'fs'), 'tp'), may hold values from -0.125 to 0.125
- state_key: bfloat16 [2048, 1024], P(('sp', 'fs'), 'tp'), may hold values from -0.125 to 0.125
- state_value: bfloat16 [2048, 1024], P(('sp', 'fs'), 'tp'), may hold values from -0.125 to 0.125
- state_decay: bfloat16 [2048, 1024], P(('sp', 'fs'), 'tp'), may hold values from -0.125 to 0.125
- state_gate: bfloat16 [2048, 1024], P(('sp', 'fs'), 'tp'), may hold values from -0.125 to 0.125
- conv_taps: float32 [31, 512], P(None, 'tp'), may hold values from -4 to 4
- conv_gain: float32 [512], P('tp'), may hold values from 0.1 to 1.9
- point_weight: bfloat16 [512, 512], replicated, may hold values from -0.25 to 0.25
- decay_base: float32 [1024], P('tp'), may hold values from -13 to -3
- correction: float32 [1024], P('tp'), may hold values from 0 to 0.9
- group_gain: float32 [1024], P('tp'), may hold values from 0.1 to 1.9
- output_conv: bfloat16 [512, 2048], P('tp', ('sp', 'fs')), may hold values from -0.25 to 0.25
- output_state: bfloat16 [1024, 2048], P('tp', ('sp', 'fs')), may hold values from -0.1875 to 0.1875
Outputs:
- mixed: bfloat16 [4, 768, 2048], P('fs', ('sp', 'tp'))
The draws below stay inside these ranges and needn't reach their ends.
Inputs may be any that keep to these rules, and one draw needn't show every extreme that they name: `decay_pace`: constant over runs of positions, a quarter of 192 long.
All inputs are finite; a program needn't handle non-finite values.
Results may differ from the reference program's by a relative error of at most 0.017.
Values may be sent and summed in bfloat16 or wider, within the bound.
No kernel may reach another device: no remote copies, remote signals or barrier semaphores. Data moves between devices by JAX's collectives and lax.ppermute only.
A program may use at most 64 MiB of HBM per device.

```python
import jax
import jax.numpy as jnp
from jax import lax

D = 2048
CB = 512
C_HEADS = 16
HEAD = 64
KERNEL = 31
TOK_DEV = 192
C = 1024
SEQ = 768
SEQS = 4


def log_uniform(key, shape, lower, upper):
    fraction = jax.random.uniform(key, shape, jnp.float32)
    return jnp.exp(jnp.log(lower) + fraction * (jnp.log(upper) - jnp.log(lower)))


def fast_channels(key):
    picks = jax.random.randint(jax.random.fold_in(key, 11), (C_HEADS,), 0, 10)
    chosen = picks < 5
    return jnp.repeat(chosen, HEAD)


def draw_decay_base(key, part):
    fast = fast_channels(key)
    slow_rate = log_uniform(jax.random.fold_in(key, 3), (C,), 0.15, 0.8) / SEQ
    fast_rate = log_uniform(jax.random.fold_in(key, 4), (C,), 0.012, 0.04)
    return jnp.clip(jnp.log(jnp.where(fast, fast_rate, slow_rate)), -13.0, -3.0)


def draw_correction(key, part):
    fast = fast_channels(key)
    slow_value = jnp.minimum(log_uniform(jax.random.fold_in(key, 5), (C,), 0.1, 0.6) * HEAD / SEQ, 0.9)
    fast_value = jax.random.uniform(jax.random.fold_in(key, 6), (C,), jnp.float32, 0.2, 0.9)
    return jnp.where(fast, fast_value, slow_value)


def draw_decay_pace(key, part):
    stretch = max(TOK_DEV // 4, 1)
    values = log_uniform(key, (SEQS, SEQ // stretch), 0.5, 2.0)
    return jnp.repeat(values, stretch, axis=1)


def draw_conv_taps(key, part):
    group = max(CB // 16, 1)
    factor = log_uniform(jax.random.fold_in(key, 8), (CB // group,), 1.0 / 3.0, 3.0)
    taps = jax.random.normal(jax.random.fold_in(key, 9), (KERNEL, CB), jnp.float32) * KERNEL ** (-0.5)
    return jnp.clip(taps * jnp.repeat(factor, group)[None, :], -4.0, 4.0)


def block_levels(key, shape, split, low, top_value):
    gain, own = 1.0, jax.random.fold_in(key, 6)
    for axis_at, blocks in split:
        heights = jnp.exp(jax.random.uniform(jax.random.fold_in(own, axis_at), (blocks,), jnp.float32, low / len(split), top_value / len(split)))
        gain = gain * jnp.repeat(heights, shape[axis_at] // blocks).reshape([-1 if axis == axis_at else 1 for axis in range(len(shape))])
    return gain


def bell_draw(stream_key, shape, scale, reach, shards=(), held_as=jnp.bfloat16):
    loudness = block_levels(stream_key, shape, shards, -0.22, 0.18) if shards else 1.0
    values = jax.random.normal(stream_key, shape, jnp.float32) * scale * loudness
    return jnp.minimum(jnp.maximum(values, -reach), reach).astype(held_as)


def setup_inputs(seed: int = 0) -> dict:
    seeds = jax.random.split(jax.random.key(seed), 21)
    return {
        "tokens": bell_draw(seeds[0], (SEQS, SEQ, D), 1.0, 6.0, ((0, 4), (1, 4))),
        "decay_pace": draw_decay_pace(jax.random.fold_in(seeds[20], 71), 0),
        "start_state": bell_draw(seeds[2], (SEQS, C_HEADS, HEAD, HEAD), (0.5 * SEQ ** 0.5), 80.0, ((0, 4), (1, 2)), jnp.float32),
        "norm_gain": jnp.clip(1.0 + 0.18 * jax.random.normal(seeds[3], (D,), jnp.float32), 0.1, 1.9),
        "conv_value": bell_draw(seeds[4], (D, CB), D ** -0.5, 0.125, ((0, 16), (1, 2))),
        "conv_admit": bell_draw(seeds[5], (D, CB), D ** -0.5, 0.125, ((0, 16), (1, 2))),
        "conv_gate": bell_draw(seeds[6], (D, CB), D ** -0.5, 0.125, ((0, 16), (1, 2))),
        "state_query": bell_draw(seeds[7], (D, C), D ** -0.5, 0.125, ((0, 16), (1, 2))),
        "state_key": bell_draw(seeds[8], (D, C), D ** -0.5, 0.125, ((0, 16), (1, 2))),
        "state_value": bell_draw(seeds[9], (D, C), D ** -0.5, 0.125, ((0, 16), (1, 2))),
        "state_decay": bell_draw(seeds[10], (D, C), D ** -0.5, 0.125, ((0, 16), (1, 2))),
        "state_gate": bell_draw(seeds[11], (D, C), D ** -0.5, 0.125, ((0, 16), (1, 2))),
        "conv_taps": draw_conv_taps(jax.random.fold_in(seeds[20], 71), 0),
        "conv_gain": jnp.clip(1.0 + 0.18 * jax.random.normal(seeds[13], (CB,), jnp.float32), 0.1, 1.9),
        "point_weight": bell_draw(seeds[14], (CB, CB), CB ** -0.5, 0.25),
        "decay_base": draw_decay_base(jax.random.fold_in(seeds[20], 71), 0),
        "correction": draw_correction(jax.random.fold_in(seeds[20], 71), 0),
        "group_gain": jnp.clip(1.0 + 0.18 * jax.random.normal(seeds[17], (C,), jnp.float32), 0.1, 1.9),
        "output_conv": bell_draw(seeds[18], (CB, D), CB ** -0.5, 0.25, ((0, 2), (1, 16))),
        "output_state": bell_draw(seeds[19], (C, D), C ** -0.5, 0.1875, ((0, 2), (1, 16))),
    }


NORM_FLOOR = 0.1
CHANNEL_FLOOR = 0.1
GROUP_FLOOR = 1.0

def project(normed_rows, weight, shape):
    return jnp.dot(normed_rows, weight, preferred_element_type=jnp.float32).astype(jnp.bfloat16).reshape(shape)

def reference(tokens, decay_pace, start_state, norm_gain, conv_value, conv_admit, conv_gate, state_query, state_key, state_value, state_decay, state_gate, conv_taps, conv_gain, point_weight, decay_base, correction, group_gain, output_conv, output_state):
    seqs, length, width = tokens.shape
    floats = tokens.astype(jnp.float32)
    inverse = lax.rsqrt(lax.optimization_barrier(jnp.mean(floats * floats, axis=-1, keepdims=True)) + NORM_FLOOR)
    normed = (floats * inverse * norm_gain).astype(jnp.bfloat16).reshape(seqs * length, width)
    conv_shape = (seqs, length, CB)
    value = project(normed, conv_value, conv_shape).astype(jnp.float32)
    admit = project(normed, conv_admit, conv_shape).astype(jnp.float32)
    gate_conv = project(normed, conv_gate, conv_shape).astype(jnp.float32)
    rounded = lax.optimization_barrier((value * jax.nn.sigmoid(admit)).astype(jnp.bfloat16))
    conv_input = rounded.astype(jnp.float32)
    padded = jnp.pad(conv_input, ((0, 0), (KERNEL - 1, 0), (0, 0)))
    conv_sum = jnp.zeros(conv_shape, jnp.float32)
    for offset in range(KERNEL):
        conv_sum = conv_sum + conv_taps[offset] * padded[:, offset:offset + length]
    mean = lax.optimization_barrier(jnp.mean(conv_sum, axis=-1, keepdims=True))
    spread = lax.optimization_barrier(jnp.mean(conv_sum * conv_sum, axis=-1, keepdims=True)) - mean * mean
    shaped = jax.nn.silu((conv_sum - mean) * lax.rsqrt(spread + CHANNEL_FLOOR) * conv_gain).astype(jnp.bfloat16)
    pointwise = jnp.dot(shaped.reshape(-1, CB), point_weight, preferred_element_type=jnp.float32).reshape(conv_shape)
    conv_out = (pointwise * jax.nn.silu(gate_conv)).astype(jnp.bfloat16)
    head_shape = (seqs, length, C_HEADS, HEAD)
    query = project(normed, state_query, head_shape).astype(jnp.float32)
    keys = project(normed, state_key, head_shape).astype(jnp.float32)
    values = project(normed, state_value, head_shape).astype(jnp.float32)
    decay_in = project(normed, state_decay, (seqs, length, C)).astype(jnp.float32)
    gate_state = project(normed, state_gate, (seqs, length, C)).astype(jnp.float32)
    log_keep = -jnp.exp(decay_base + jnp.tanh(decay_in)) * decay_pace[:, :, None]
    keep = jnp.exp(log_keep).reshape(head_shape)
    unit = keys * lax.rsqrt(jnp.maximum(lax.optimization_barrier(jnp.sum(keys * keys, axis=-1, keepdims=True)), 1.0))
    remove = -unit
    write = unit * correction.reshape(C_HEADS, HEAD)

    def advance(state, inputs):
        query_now, keep_now, key_now, value_now, remove_now, write_now = inputs
        removed = jnp.einsum('shvk,shk->shv', state, remove_now, precision=lax.Precision.HIGHEST)
        state = state * keep_now[:, :, None, :] + removed[..., None] * write_now[:, :, None, :] + value_now[..., None] * key_now[:, :, None, :]
        return (state, jnp.einsum('shvk,shk->shv', state, query_now, precision=lax.Precision.HIGHEST))
    inputs = tuple((jnp.moveaxis(array, 1, 0) for array in (query, keep, keys, values, remove, write)))
    final_state, outputs = lax.scan(advance, start_state.astype(jnp.float32), inputs)
    outputs = jnp.moveaxis(outputs, 0, 1)
    centered = outputs - lax.optimization_barrier(jnp.mean(outputs, axis=-1, keepdims=True))
    variance = lax.optimization_barrier(jnp.mean(centered * centered, axis=-1, keepdims=True))
    grouped = centered * lax.rsqrt(variance + GROUP_FLOOR) * group_gain.reshape(C_HEADS, HEAD)
    state_out = (grouped.reshape(seqs, length, C) * jax.nn.silu(gate_state)).astype(jnp.bfloat16)
    joined = jnp.concatenate([conv_out, state_out], axis=-1).reshape(seqs * length, CB + C)
    weight = jnp.concatenate([output_conv, output_state], axis=0)
    mixed = jnp.dot(joined, weight, preferred_element_type=jnp.float32).astype(jnp.bfloat16)
    return mixed.reshape(seqs, length, width)
```

```python
import functools

import jax
import jax.numpy as jnp
from jax import lax
from jax.experimental import pallas as pl
from jax.experimental.pallas import tpu as pltpu
from jax.sharding import PartitionSpec as P

NORM_FLOOR = 0.1
CHANNEL_FLOOR = 0.1
GROUP_FLOOR = 1.0
LANES = 128
SPAN = 64
BF = jnp.bfloat16
F32 = jnp.float32
ANY = pl.BlockSpec(memory_space=pl.ANY)
VM = pl.BlockSpec(memory_space=pltpu.VMEM)
SM = pl.BlockSpec(memory_space=pltpu.SMEM)


def dot_nn(a, b):
    return lax.dot_general(a, b, (((1,), (0,)), ((), ())), preferred_element_type=F32)


def dot_nt(a, b):
    return lax.dot_general(a, b, (((1,), (1,)), ((), ())), preferred_element_type=F32)


def dot_tn(a, b):
    return lax.dot_general(a, b, (((0,), (0,)), ((), ())), preferred_element_type=F32)


def sigmoid(x):
    return 1.0 / (1.0 + jnp.exp(-x))


def iota(shape, dim):
    return lax.broadcasted_iota(jnp.int32, shape, dim)


def split_weights_kernel(place, *refs):
    convs, states, outs = refs[:3], refs[3:8], refs[8:]
    count = len(outs)
    half = LANES // 2
    for step, out in enumerate(outs):
        target = lax.rem(place[0] + step, count)
        for at, ref in enumerate(states):
            out[:, at * LANES : (at + 1) * LANES] = ref[
                :, pl.ds(pl.multiple_of(target * LANES, LANES), LANES)
            ]
        odd = lax.rem(target, 2) == 1
        for at, ref in enumerate(convs):
            pair = ref[:, pl.ds(pl.multiple_of((target // 2) * LANES, LANES), LANES)]
            start = len(states) * LANES + at * half
            out[:, start : start + half] = jnp.where(odd, pair[:, half:], pair[:, :half])


def norm_kernel(place, tokens, gain, out_conv, out_state, normed, part, rows_out):
    count = part.shape[0]
    floats = tokens[...].astype(F32)
    inverse = lax.rsqrt(jnp.mean(floats * floats, axis=1, keepdims=True) + NORM_FLOOR)
    normed[...] = (floats * inverse * gain[...]).astype(BF)
    part[...] = normed[pl.ds(pl.multiple_of(place[0] * count, 16), count), :]
    split = out_conv.shape[0]
    rows_out[:split, :] = out_conv[...]
    rows_out[split:, :] = out_state[...]


def assemble_kernel(*refs):
    *sources, out, sem = refs
    copies = [pltpu.make_async_copy(s, out.at[i], sem.at[i]) for i, s in enumerate(sources)]
    for copy in copies:
        copy.start()
    for copy in copies:
        copy.wait()


def assemble(*arrays):
    return pl.pallas_call(
        assemble_kernel,
        out_shape=jax.ShapeDtypeStruct((len(arrays),) + arrays[0].shape, arrays[0].dtype),
        in_specs=[ANY] * len(arrays),
        out_specs=ANY,
        scratch_shapes=[pltpu.SemaphoreType.DMA((len(arrays),))],
        name="assemble",
    )(*arrays)


def mixer_kernel(
    place, pace, own, *refs, length, halves, blocks_order
):
    near = refs[: len(blocks_order)]
    far = refs[len(blocks_order) : 2 * len(blocks_order)]
    (
        mine, sibling, start, base, correction, group_gain, taps, out,
        x, w, proj, log_keep, conv_rows, y, sems,
    ) = refs[2 * len(blocks_order) :]
    z, f, t = place[0], place[1], place[2]
    total_rows = x.shape[0]
    count = total_rows // length
    part = length // halves
    jobs = []
    slot = 0
    for i in range(mine.shape[0]):
        level, step = i // count, i % count
        source = lax.rem(z - step + count, count)
        for ref, flip in ((mine, 0), (sibling, 1)):
            row = (source * count + (f ^ (2 * level) ^ flip)) * LANES
            jobs.append(
                (None, pltpu.make_async_copy(
                    ref.at[i], w.at[pl.ds(pl.multiple_of(row, LANES), LANES), :], sems.at[slot]
                ))
            )
            slot += 1
    jobs.append(
        (None, pltpu.make_async_copy(
            own, x.at[pl.ds(pl.multiple_of(z * length, 64), length), :], sems.at[slot]
        ))
    )
    slot += 1
    for (offset, valid), a, b in zip(blocks_order, near, far):
        position = offset(z)
        for ref, half in ((a, t), (b, 1 - t)):
            row = pl.multiple_of(position * length + half * part, 32)
            jobs.append(
                (valid(z), pltpu.make_async_copy(ref, x.at[pl.ds(row, part), :], sems.at[slot]))
            )
            slot += 1
    for condition, copy in jobs:
        if condition is None:
            copy.start()
        else:
            pl.when(condition)(copy.start)
    for condition, copy in jobs:
        if condition is None:
            copy.wait()
        else:
            pl.when(condition)(copy.wait)

    half = LANES // 2
    lane = iota((1, LANES), 1)
    first = (lane < half).astype(F32)
    second = 1.0 - first
    ri, ci = iota((LANES, LANES), 0), iota((LANES, LANES), 1)
    same = (ri // half) == (ci // half)
    mean_mat = jnp.where(same, 1.0 / half, 0.0).astype(BF)
    sum_mat = jnp.where(same, 1.0, 0.0).astype(BF)
    strict = same & (ri > ci)
    weak = same & (ri >= ci)
    eye = jnp.where(ri == ci, 1.0, 0.0).astype(F32)

    run = length // 4
    column = pl.ds(pl.multiple_of(z * LANES, LANES), LANES)
    base_row = base[:, column]
    for block in range(count):
        rows = slice(block * length, (block + 1) * length)
        proj[rows, :] = dot_nn(x[rows, :], w[...]).astype(BF)
        decay_in = proj[rows, 3 * LANES : 4 * LANES].astype(F32)
        rate = -jnp.exp(base_row + jnp.tanh(decay_in))
        for r in range(4):
            log_keep[block * length + r * run : block * length + (r + 1) * run, :] = (
                rate[r * run : (r + 1) * run, :] * pace[block * 4 + r]
            )

    left = 5 * LANES
    pair = proj[:, left : left + LANES].astype(F32)
    conv_in = (pair * pltpu.roll(sigmoid(pair), half, 1)).astype(BF).astype(F32)
    middle = total_rows // 2
    pad = conv_rows.shape[0] - middle
    moved = pltpu.roll(conv_in[middle - pad :, :], half, 1)
    conv_rows[:pad, :] = moved[:pad, :] * second
    conv_rows[pad:, :] = conv_in[:middle, :] * first + moved[pad:, :] * second
    kernel = taps.shape[0]
    tap = taps[:, pl.ds(pl.multiple_of((z // 2) * LANES, LANES), LANES)]
    turned = pltpu.roll(tap, half, 1)
    odd = (lax.rem(z, 2) == 1).astype(F32)
    tap = jnp.where((lane < half) == (odd < 0.5), tap, turned)
    lead = pad - (kernel - 1)
    strip = 96
    for at in range(0, middle, strip):
        total = jnp.zeros((strip, LANES), F32)
        for j in range(kernel):
            total = total + tap[j : j + 1, :] * conv_rows[at + lead + j : at + lead + j + strip, :]
        total = total.astype(BF)
        out[at : at + strip, LANES : LANES + half] = total[:, :half]
        out[middle + at : middle + at + strip, LANES : LANES + half] = total[:, half:]
    out[:, LANES + half : 2 * LANES] = proj[:, left + LANES : left + LANES + half]

    chunks = total_rows // SPAN
    corr_row = correction[:, column]
    tri = jnp.where(iota((SPAN, SPAN), 0) >= iota((SPAN, SPAN), 1), 1.0, 0.0).astype(F32)

    def stack(a):
        return jnp.concatenate([a * first, a * second], axis=0).astype(BF)

    sums = lax.dot_general(
        tri,
        jnp.concatenate([log_keep[c * SPAN : (c + 1) * SPAN, :] for c in range(chunks)], axis=1),
        (((1,), (0,)), ((), ())),
        precision=lax.Precision.HIGHEST,
        preferred_element_type=F32,
    )
    levels = []
    size = 1
    while size < SPAN:
        inside = (ri // (2 * size)) == (ci // (2 * size))
        levels.append(inside & ((ri & size) != 0) & ((ci & size) == 0))
        size *= 2

    group = 6
    carried = []
    for at in range(0, chunks, group):
        members = list(range(at, min(at + group, chunks)))
        grams, tails, heads = [], [], []
        for c in members:
            rows = slice(c * SPAN, (c + 1) * SPAN)
            total = sums[:, c * LANES : (c + 1) * LANES]
            before = total - log_keep[rows, :]
            last = total[SPAN - 1 : SPAN, :]
            q = proj[rows, 0:LANES].astype(F32)
            k = proj[rows, LANES : 2 * LANES].astype(F32)
            v = proj[rows, 2 * LANES : 3 * LANES].astype(F32)
            norm = dot_nn((k * k).astype(BF), sum_mat)
            unit = k * lax.rsqrt(jnp.maximum(norm, 1.0))
            write = unit * corr_row
            back = jnp.exp(-total)
            rest = jnp.exp(last - total)
            lead_remove = stack(-unit * jnp.exp(before))
            lead_query = stack(q * jnp.exp(total))
            grams.append(
                dot_nt(
                    jnp.concatenate([lead_remove, lead_query], axis=0),
                    jnp.concatenate([stack(write * back), stack(k * back)], axis=0),
                )
            )
            tails.append((stack(write * rest), stack(k * rest), jnp.exp(last)))
            heads.append((lead_remove, lead_query, stack(v)))
        system = [jnp.where(strict, g[:LANES, :LANES], 0.0) for g in grams]
        inverse = [eye + jnp.where(levels[0], a, 0.0) for a in system]
        for level in levels[1:]:
            low = [i.astype(BF) for i in inverse]
            inner = [
                dot_nn(i, jnp.where(level, a, 0.0).astype(BF)).astype(BF) for i, a in zip(low, system)
            ]
            inverse = [i + dot_nn(n, b) for i, n, b in zip(inverse, inner, low)]
        direct = [
            dot_nn(
                jnp.concatenate(
                    [
                        jnp.where(strict, g[:LANES, LANES:], 0.0),
                        jnp.where(weak, g[LANES:, LANES:], 0.0),
                    ],
                    axis=0,
                ).astype(BF),
                h[2],
            )
            for g, h in zip(grams, heads)
        ]
        solved = [
            dot_nn(i.astype(BF), jnp.concatenate([d[:LANES].astype(BF), h[0]], axis=1)).astype(BF)
            for i, d, h in zip(inverse, direct, heads)
        ]
        through = [
            dot_nn(jnp.where(weak, g[LANES:, :LANES], 0.0).astype(BF), s) for g, s in zip(grams, solved)
        ]
        for g, d, s, h, u, tail in zip(grams, direct, solved, heads, through, tails):
            local = u[:, :LANES] + d[LANES:]
            moved = dot_tn(s, tail[0])
            carried.append(
                (
                    local[:SPAN] + local[SPAN:],
                    (h[1].astype(F32) + u[:, LANES:]).astype(BF),
                    moved[LANES:].astype(BF),
                    moved[:LANES] + dot_tn(h[2], tail[1]),
                    tail[2],
                )
            )
    zero = jnp.zeros((half, half), F32)
    state = jnp.concatenate(
        [
            jnp.concatenate([start[2 * z], zero], axis=1),
            jnp.concatenate([zero, start[2 * z + 1]], axis=1),
        ],
        axis=0,
    )
    for c, (local, lead, step, added, kept) in enumerate(carried):
        low = state.astype(BF)
        seen = dot_nt(lead, low)
        y[c * SPAN : (c + 1) * SPAN, :] = local + seen[:SPAN] + seen[SPAN:]
        state = state * kept + dot_nn(low, step) + added

    gain_row = group_gain[:, column]
    for block in range(count):
        rows = slice(block * length, (block + 1) * length)
        values = y[rows, :]
        high = values.astype(BF)
        low = (values - high.astype(F32)).astype(BF)
        centered = values - (dot_nn(high, mean_mat) + dot_nn(low, mean_mat))
        variance = dot_nn((centered * centered).astype(BF), mean_mat)
        gate = proj[rows, 4 * LANES : 5 * LANES].astype(F32)
        grouped = centered * lax.rsqrt(variance + GROUP_FLOOR) * gain_row
        out[rows, :LANES] = (grouped * (gate * sigmoid(gate))).astype(BF)


def output_kernel(place, received, gain, point, *refs, groups):
    pieces, (out, w, sems) = refs[:-3], refs[-3:]
    z, f, t = place[0], place[1], place[2]
    sources, rows, _ = received.shape
    count = sources // groups
    half = LANES // 2
    split = count * half
    wide = count * LANES
    jobs = []
    slot = 0
    for at, piece in enumerate(pieces):
        core, flip, side = at & 1, (at >> 1) & 1, (at >> 2) & 1
        group = t ^ side
        for block in range(count):
            col = pl.multiple_of((block * count + (f ^ (2 * flip) ^ core)) * LANES, LANES)
            for start, size, shift in (
                (0, split, group * split),
                (split, wide, groups * split + group * wide),
            ):
                copy = pltpu.make_async_copy(
                    piece.at[block, pl.ds(start, size), :],
                    w.at[pl.ds(pl.multiple_of(shift, LANES), size), pl.ds(col, LANES)],
                    sems.at[slot],
                )
                copy.start()
                jobs.append(copy)
                slot += 1
    sums, gates, states = [], [], []
    for group in range(groups):
        for block in range(count):
            source = received[block * groups + group]
            states.append(source[:, :LANES])
            sums.append(source[:, LANES : LANES + half])
            gates.append(source[:, LANES + half :])
    conv_sum = jnp.concatenate(sums, axis=1).astype(F32)
    gate = jnp.concatenate(gates, axis=1).astype(F32)
    mean = jnp.mean(conv_sum, axis=1, keepdims=True)
    spread = jnp.mean(conv_sum * conv_sum, axis=1, keepdims=True) - mean * mean
    scaled = (conv_sum - mean) * lax.rsqrt(spread + CHANNEL_FLOOR) * gain[...]
    shaped = (scaled * sigmoid(scaled)).astype(BF)
    conv_out = (dot_nn(shaped, point[...]) * (gate * sigmoid(gate))).astype(BF)
    joined = jnp.concatenate([conv_out] + states, axis=1)
    for copy in jobs:
        copy.wait()
    out[...] = dot_nn(joined, w[...]).astype(BF)


def ordered_kernel(place, *refs, blocks_order):
    *sources, out, sems = refs
    z = place[0]
    jobs = [(None, pltpu.make_async_copy(sources[0], out.at[z], sems.at[0]))]
    for i, ((offset, valid), source) in enumerate(zip(blocks_order, sources[1:])):
        jobs.append(
            (valid(z), pltpu.make_async_copy(source, out.at[offset(z)], sems.at[i + 1]))
        )
    for condition, copy in jobs:
        if condition is None:
            copy.start()
        else:
            pl.when(condition)(copy.start)
    for condition, copy in jobs:
        if condition is None:
            copy.wait()
        else:
            pl.when(condition)(copy.wait)


LINE = (
    ((0, 1), (1, 2), (2, 3)),
    ((1, 0), (2, 1), (3, 2)),
    ((0, 2), (1, 3), (2, 0), (3, 1)),
    ((2, 3), (1, 0)),
)
LINE_ORDER = (
    (lambda z: jnp.maximum(z - 1, 0), lambda z: z > 0),
    (lambda z: jnp.minimum(z + 1, 3), lambda z: z < 3),
    (lambda z: z ^ 2, lambda z: z >= 0),
    (lambda z: z ^ 3, lambda z: (z == 0) | (z == 3)),
)


def along_line(value):
    right, left, double = (lax.ppermute(value, "sp", LINE[i]) for i in range(3))
    return right, left, double, lax.ppermute(double, "sp", LINE[3])


def across(value, pairs):
    targets = sorted({b for _, b in pairs})
    return lax.ppermute(
        value, ("sp", "tp"), [(2 * i + s, 2 * i + 1 - s) for i in targets for s in (0, 1)]
    )


def flipped(value, axis, bit):
    count = lax.axis_size(axis)
    return lax.ppermute(value, axis, [(i, i ^ bit) for i in range(count)])


def head_body(
    tokens, decay_pace, start_state, norm_gain, conv_value, conv_admit, conv_gate, state_query,
    state_key, state_value, state_decay, state_gate, conv_taps, conv_gain, point_weight, decay_base,
    correction, group_gain, output_conv, output_state,
):
    width = tokens.shape[-1]
    length = tokens.shape[1]
    count, halves = lax.axis_size("sp"), lax.axis_size("tp")
    part = length // halves
    place = jnp.stack([lax.axis_index(a) for a in ("sp", "fs", "tp")]).astype(jnp.int32)
    shard = conv_value.shape[0]
    columns = 5 * LANES + 3 * LANES // 2
    slices = pl.pallas_call(
        split_weights_kernel,
        out_shape=[jax.ShapeDtypeStruct((shard, columns), BF)] * count,
        in_specs=[SM] + [VM] * 8,
        out_specs=[VM] * count,
        name="split_weights",
    )(place, conv_value, conv_admit, conv_gate, state_query, state_key, state_value, state_decay, state_gate)
    taken = [slices[0]] + [
        lax.ppermute(slices[k], "sp", [(s, (s + k) % count) for s in range(count)])
        for k in range(1, count)
    ]
    out_rows = output_conv.shape[0] + output_state.shape[0]
    normed, half, rows_out = pl.pallas_call(
        norm_kernel,
        out_shape=[
            jax.ShapeDtypeStruct((length, width), BF),
            jax.ShapeDtypeStruct((part, width), BF),
            jax.ShapeDtypeStruct((out_rows, output_conv.shape[1]), BF),
        ],
        in_specs=[SM, VM, VM, VM, VM],
        out_specs=[VM] * 3,
        name="norm",
    )(place[2:], tokens.reshape(length, width), norm_gain.reshape(1, width), output_conv, output_state)
    near = along_line(half)
    far = [across(a, LINE[i]) for i, a in enumerate(near)]
    lifted = [flipped(a, "fs", 2) for a in taken]
    mine = assemble(*taken, *lifted)
    sibling = flipped(mine, "fs", 1)
    paces = lax.all_gather(decay_pace[0, :: length // 4], "sp", axis=0, tiled=True)
    gain_other = flipped(conv_gain, "tp", 1)
    low = lax.axis_index("tp") == 0
    gain = jnp.concatenate(
        [jnp.where(low, conv_gain, gain_other), jnp.where(low, gain_other, conv_gain)]
    )
    line_out = along_line(rows_out)
    ordered = pl.pallas_call(
        functools.partial(ordered_kernel, blocks_order=LINE_ORDER),
        out_shape=jax.ShapeDtypeStruct((count,) + rows_out.shape, BF),
        in_specs=[SM] + [ANY] * 5,
        out_specs=ANY,
        scratch_shapes=[pltpu.SemaphoreType.DMA((5,))],
        name="ordered",
    )(place, rows_out, *line_out)
    crossed = flipped(ordered, "tp", 1)
    pieces = []
    for a in (ordered, crossed):
        for b in (a, flipped(a, "fs", 2)):
            pieces += [b, flipped(b, "fs", 1)]
    total = length * count
    rows = total // (count * halves)
    heads = start_state.shape[1]
    mixed = pl.pallas_call(
        functools.partial(mixer_kernel, length=length, halves=halves, blocks_order=LINE_ORDER),
        out_shape=jax.ShapeDtypeStruct((total, 2 * LANES), BF),
        in_specs=[SM, SM] + [ANY] * 11 + [VM] * 5,
        out_specs=VM,
        scratch_shapes=[
            pltpu.VMEM((total, width), BF),
            pltpu.VMEM((width, columns), BF),
            pltpu.VMEM((total, columns), BF),
            pltpu.VMEM((total, LANES), F32),
            pltpu.VMEM((total // 2 + 32, LANES), F32),
            pltpu.VMEM((total, LANES), F32),
            pltpu.SemaphoreType.DMA((32,)),
        ],
        name="mixer",
    )(
        place, paces, normed, *near, *far, mine, sibling,
        start_state.reshape(heads, *start_state.shape[2:]),
        decay_base.reshape(1, -1), correction.reshape(1, -1), group_gain.reshape(1, -1), conv_taps,
    )
    received = lax.all_to_all(
        mixed.reshape(count * halves, rows, 2 * LANES), ("sp", "tp"), 0, 0, tiled=True
    )
    out = pl.pallas_call(
        functools.partial(output_kernel, groups=halves),
        out_shape=jax.ShapeDtypeStruct((rows, width), BF),
        in_specs=[SM, VM, VM, VM] + [ANY] * 8,
        out_specs=VM,
        scratch_shapes=[
            pltpu.VMEM((halves * out_rows, width), BF),
            pltpu.SemaphoreType.DMA((64,)),
        ],
        name="output",
    )(place, received, gain.reshape(1, -1), point_weight, *pieces)
    return out.reshape(1, rows, width)


def passed_along(value, axis, steps):
    count = lax.axis_size(axis)
    leading, last = (max(0, -steps), min(count, count - steps))
    return lax.ppermute(value, axis, [(source, source + steps) for source in range(leading, last)])


def entering_2(value, axis, join, neutral):
    place = lax.axis_index(axis)
    gathered = jax.tree.map(
        lambda a, kind: lax.all_gather(a.astype(kind), axis),
        value,
        jax.tree.map(lambda a: jnp.bfloat16 if a.dtype == jnp.float32 else a.dtype, value),
    )
    state = jax.tree.map(lambda a, e: jnp.zeros_like(a) + jnp.asarray(e, a.dtype), value, neutral)

    def one(lap, state):
        return join(
            state,
            jax.tree.map(
                lambda a, own: lax.dynamic_index_in_dim(a, lap, 0, False).astype(own.dtype),
                gathered,
                value,
            ),
        )

    return lax.fori_loop(0, place, one, state)


def apply_map(matrix, right):
    return jnp.einsum("hbti,hbic->hbtc", matrix, right, precision=lax.Precision.HIGHEST)


def pair_terms(left, right, mask):
    return jnp.einsum("hbtc,hbic->hbti", left, right, precision=lax.Precision.HIGHEST) * mask


def compose(earlier, later):
    first = jnp.matmul(earlier[0], later[0], precision=lax.Precision.HIGHEST)
    second = jnp.matmul(earlier[1], later[0], precision=lax.Precision.HIGHEST) + later[1]
    return (first, second)


def block_terms(query, keys, values, unit, write, log_keep):
    size = query.shape[-1]
    span = query.shape[2]
    total_log = jnp.cumsum(log_keep, axis=2)
    before_log = total_log - log_keep
    last_log = total_log[:, :, span - 1 :, :]
    lead_remove = -unit * jnp.exp(before_log)
    lead_query = query * jnp.exp(total_log)
    back_write = write * jnp.exp(-total_log)
    back_key = keys * jnp.exp(-total_log)
    places = jnp.arange(span)
    strict = (places[:, None] > places[None, :]).astype(jnp.float32)
    weak = (places[:, None] >= places[None, :]).astype(jnp.float32)
    remove_write = pair_terms(lead_remove, back_write, strict)
    remove_key = pair_terms(lead_remove, back_key, strict)
    query_write = pair_terms(lead_query, back_write, weak)
    query_key = pair_terms(lead_query, back_key, weak)
    right_side = jnp.concatenate([apply_map(remove_key, values), lead_remove], axis=-1)
    system = jnp.eye(span, dtype=jnp.float32) - remove_write
    solved = jax.scipy.linalg.solve_triangular(system, right_side, lower=True, unit_diagonal=True)
    own_part = solved[..., :size]
    start_part = solved[..., size:]
    local_out = apply_map(query_write, own_part) + apply_map(query_key, values)
    start_map = lead_query + apply_map(query_write, start_part)
    tail_write = write * jnp.exp(last_log - total_log)
    tail_key = keys * jnp.exp(last_log - total_log)
    carry_map = jnp.einsum(
        "hbtk,hbtj->hbkj", start_part, tail_write, precision=lax.Precision.HIGHEST
    ) + jnp.eye(size, dtype=jnp.float32) * jnp.exp(last_log)
    carry_add = jnp.einsum(
        "hbtv,hbtj->hbvj", own_part, tail_write, precision=lax.Precision.HIGHEST
    ) + jnp.einsum("hbtv,hbtj->hbvj", values, tail_key, precision=lax.Precision.HIGHEST)
    return (local_out, start_map, carry_map, carry_add)


def body(
    tokens,
    decay_pace,
    start_state,
    norm_gain,
    conv_value,
    conv_admit,
    conv_gate,
    state_query,
    state_key,
    state_value,
    state_decay,
    state_gate,
    conv_taps,
    conv_gain,
    point_weight,
    decay_base,
    correction,
    group_gain,
    output_conv,
    output_state,
):
    width = tokens.shape[-1]
    rows = tokens.reshape(-1, width)
    length = rows.shape[0]
    floats = rows.astype(jnp.float32)
    inverse = lax.rsqrt(jnp.mean(floats * floats, axis=1, keepdims=True) + NORM_FLOOR)
    normed = (floats * inverse * norm_gain).astype(jnp.bfloat16)
    shards = (
        conv_value,
        conv_admit,
        conv_gate,
        state_query,
        state_key,
        state_value,
        state_decay,
        state_gate,
    )
    stacked = jnp.concatenate(shards, axis=1)
    projected = jnp.dot(
        normed,
        lax.all_gather(stacked, ("sp", "fs"), axis=0, tiled=True),
        preferred_element_type=jnp.float32,
    ).astype(jnp.bfloat16)
    pieces = []
    offset = 0
    for shard in shards:
        pieces.append(projected[:, offset : offset + shard.shape[1]].astype(jnp.float32))
        offset = offset + shard.shape[1]
    value, admit, gate_conv, query, keys, values, decay_in, gate_state = pieces
    channels = value.shape[1]
    kernel = conv_taps.shape[0]
    conv_input = (value * jax.nn.sigmoid(admit)).astype(jnp.bfloat16)
    earlier = passed_along(conv_input[length - (kernel - 1) :], "sp", 1)
    padded = jnp.concatenate([earlier, conv_input], axis=0).astype(jnp.float32)
    conv_sum = jnp.zeros((length, channels), jnp.float32)
    for place in range(kernel):
        conv_sum = conv_sum + conv_taps[place] * padded[place : place + length]
    local_point = lax.dynamic_slice_in_dim(
        point_weight, lax.axis_index("tp") * channels, channels, 1
    )
    whole_sum, whole_gain = (
        lax.all_gather(conv_sum.astype(jnp.bfloat16), "tp", axis=1, tiled=True).astype(
            conv_sum.dtype
        ),
        lax.all_gather(conv_gain.astype(jnp.bfloat16), "tp", axis=0, tiled=True).astype(
            conv_gain.dtype
        ),
    )
    mean = jnp.mean(whole_sum, axis=1, keepdims=True)
    spread = jnp.mean(whole_sum * whole_sum, axis=1, keepdims=True) - mean * mean
    shaped = jax.nn.silu(
        (whole_sum - mean) * lax.rsqrt(spread + CHANNEL_FLOOR) * whole_gain
    ).astype(jnp.bfloat16)
    pointwise = jnp.dot(shaped, local_point, preferred_element_type=jnp.float32)
    conv_out = (pointwise * jax.nn.silu(gate_conv)).astype(jnp.bfloat16)
    size = start_state.shape[-1]
    heads = query.shape[1] // size
    span = min(64, length)
    blocks = length // span
    log_keep = -jnp.exp(decay_base + jnp.tanh(decay_in)) * decay_pace.reshape(-1)[:, None]
    key_heads = keys.reshape(length, heads, size)
    unit = key_heads * lax.rsqrt(
        jnp.maximum(jnp.sum(key_heads * key_heads, axis=-1, keepdims=True), 1.0)
    )
    write = unit * correction.reshape(heads, size)

    def arrange(array):
        return array.reshape(blocks, span, heads, size).transpose(2, 0, 1, 3)

    local_out, start_map, carry_map, carry_add = block_terms(
        arrange(query),
        arrange(keys),
        arrange(values),
        arrange(unit),
        arrange(write),
        arrange(log_keep),
    )
    identity = (
        jnp.broadcast_to(jnp.eye(size, dtype=jnp.float32), (heads, size, size)),
        jnp.zeros((heads, size, size), jnp.float32),
    )

    def along(carried, block_pair):
        return (compose(carried, block_pair), carried)

    device_pair, prefixes = lax.scan(
        along, identity, (jnp.moveaxis(carry_map, 1, 0), jnp.moveaxis(carry_add, 1, 0))
    )
    prior_map, prior_add = entering_2(device_pair, "sp", compose, identity)
    begin = start_state.reshape(heads, size, size)
    entering = jnp.matmul(begin, prior_map, precision=lax.Precision.HIGHEST) + prior_add
    block_starts = (
        jnp.matmul(entering[None], prefixes[0], precision=lax.Precision.HIGHEST) + prefixes[1]
    )
    block_starts = jnp.moveaxis(block_starts, 0, 1)
    outputs = local_out + jnp.einsum(
        "hbtk,hbvk->hbtv", start_map, block_starts, precision=lax.Precision.HIGHEST
    )
    outputs = outputs.transpose(1, 2, 0, 3).reshape(length, heads, size)
    centered = outputs - jnp.mean(outputs, axis=-1, keepdims=True)
    variance = jnp.mean(centered * centered, axis=-1, keepdims=True)
    grouped = centered * lax.rsqrt(variance + GROUP_FLOOR) * group_gain.reshape(heads, size)
    state_out = (grouped.reshape(length, heads * size) * jax.nn.silu(gate_state)).astype(
        jnp.bfloat16
    )
    local_mix = jnp.concatenate([conv_out, state_out], axis=1)
    moved = lax.all_to_all(local_mix, "tp", split_axis=0, concat_axis=1, tiled=True)
    conv_rows, state_rows = (
        lax.all_gather(output_conv, "tp", axis=0, tiled=True),
        lax.all_gather(output_state, "tp", axis=0, tiled=True),
    )
    groups = lax.axis_size("tp")
    joined = jnp.concatenate(
        [conv_rows.reshape(groups, channels, -1), state_rows.reshape(groups, heads * size, -1)],
        axis=1,
    )
    joined = joined.reshape(groups * (channels + heads * size), -1)
    mixed = jnp.dot(
        moved,
        lax.all_gather(joined, ("sp", "fs"), axis=1, tiled=True),
        preferred_element_type=jnp.float32,
    )
    return mixed.astype(jnp.bfloat16).reshape(1, -1, width)


def layer(*args):
    sizes = [lax.axis_size(a) for a in ("sp", "fs", "tp")]
    channels, wide = args[4].shape[1], args[7].shape[1]
    whole = channels == sizes[0] * LANES // 2 and wide == sizes[0] * LANES
    square = args[2].shape[-1] == LANES // 2 and args[4].shape[0] == LANES
    return (head_body if sizes == [4, 4, 2] and whole and square else body)(*args)


def solution(mesh):
    return jax.shard_map(
        layer,
        mesh=mesh,
        in_specs=(
            P("fs", "sp", None),
            P("fs", "sp"),
            P("fs", "tp", None, None),
            P(),
            P(("sp", "fs"), "tp"),
            P(("sp", "fs"), "tp"),
            P(("sp", "fs"), "tp"),
            P(("sp", "fs"), "tp"),
            P(("sp", "fs"), "tp"),
            P(("sp", "fs"), "tp"),
            P(("sp", "fs"), "tp"),
            P(("sp", "fs"), "tp"),
            P(None, "tp"),
            P("tp"),
            P(),
            P("tp"),
            P("tp"),
            P("tp"),
            P("tp", ("sp", "fs")),
            P("tp", ("sp", "fs")),
        ),
        out_specs=P("fs", ("sp", "tp"), None),
        check_vma=False,
    )
```

```python
import functools

import jax
import jax.numpy as jnp
from jax import lax
from jax.experimental import pallas as pl
from jax.experimental.pallas import tpu as pltpu
from jax.sharding import PartitionSpec as P

NORM_FLOOR = 0.1
CHANNEL_FLOOR = 0.1
GROUP_FLOOR = 1.0
LANES = 128
SPAN = 64
SPARE = 32
BF = jnp.bfloat16
F32 = jnp.float32
VM = pl.BlockSpec(memory_space=pltpu.VMEM)
SM = pl.BlockSpec(memory_space=pltpu.SMEM)


def dot_nn(a, b):
    return lax.dot_general(a, b, (((1,), (0,)), ((), ())), preferred_element_type=F32)


def dot_nt(a, b):
    return lax.dot_general(a, b, (((1,), (1,)), ((), ())), preferred_element_type=F32)


def dot_tn(a, b):
    return lax.dot_general(a, b, (((0,), (0,)), ((), ())), preferred_element_type=F32)


def sigmoid(x):
    return 1.0 / (1.0 + jnp.exp(-x))


def iota(shape, dim):
    return lax.broadcasted_iota(jnp.int32, shape, dim)


def split_weights_kernel(place, *refs):
    convs, states, outs = refs[:3], refs[3:8], refs[8:]
    count = len(outs)
    half = LANES // 2
    for step, out in enumerate(outs):
        target = lax.rem(place[0] + step, count)
        for at, ref in enumerate(states):
            out[:, at * LANES : (at + 1) * LANES] = ref[
                :, pl.ds(pl.multiple_of(target * LANES, LANES), LANES)
            ]
        odd = lax.rem(target, 2) == 1
        for at, ref in enumerate(convs):
            pair = ref[:, pl.ds(pl.multiple_of((target // 2) * LANES, LANES), LANES)]
            start = len(states) * LANES + at * half
            out[:, start : start + half] = jnp.where(odd, pair[:, half:], pair[:, :half])
        out[:, start + half :] = jnp.zeros((out.shape[0], half), BF)


def three_terms(a):
    high = a.astype(BF).astype(F32)
    middle = (a - high).astype(BF).astype(F32)
    return high, middle, a - high - middle


def norm_kernel(place, tokens, gain, out_conv, out_state, pace, conv_gain, normed, part, rows_out):
    count = part.shape[0]
    floats = tokens[...].astype(F32)
    inverse = lax.rsqrt(jnp.mean(floats * floats, axis=1, keepdims=True) + NORM_FLOOR)
    normed[...] = (floats * inverse * gain[...]).astype(BF)
    part[...] = normed[pl.ds(pl.multiple_of(place[0] * count, 16), count), :]
    split, wide = out_conv.shape[0], out_state.shape[0]
    rows_out[:split, :] = out_conv[...]
    rows_out[split : split + wide, :] = out_state[...]
    run = pace.shape[1] // 4
    paces = jnp.concatenate(
        [jnp.broadcast_to(pace[:, r * run : r * run + 1], (1, LANES)) for r in range(4)], axis=0
    )
    gains = jnp.concatenate(
        [conv_gain[:, i * LANES : (i + 1) * LANES] for i in range(split // LANES)], axis=0
    )
    spare = jnp.concatenate(
        list(three_terms(paces))
        + list(three_terms(gains))
        + [jnp.zeros((SPARE - 12 - 3 * gains.shape[0], LANES), F32)],
        axis=0,
    )
    rows_out[split + wide :, :] = spare.astype(BF)


def assemble_kernel(*refs):
    *sources, out = refs
    size = sources[0].shape[0]
    for i, source in enumerate(sources):
        out[i * size : (i + 1) * size, :] = source[...]


def assemble(*arrays):
    return pl.pallas_call(
        assemble_kernel,
        out_shape=jax.ShapeDtypeStruct(
            (len(arrays) * arrays[0].shape[0], arrays[0].shape[1]), arrays[0].dtype
        ),
        in_specs=[VM] * len(arrays),
        out_specs=VM,
        name="assemble",
    )(*arrays)


def mixer_kernel(place, own, *refs, length, halves, blocks_order):
    near = refs[: len(blocks_order)]
    far = refs[len(blocks_order) : 2 * len(blocks_order)]
    (
        mine, sibling, shards, start, base, correction, group_gain, taps, out,
        x, w, proj, log_keep, conv_rows, y,
    ) = refs[2 * len(blocks_order) :]
    z, f, t = place[0], place[1], place[2]
    total_rows = x.shape[0]
    count = total_rows // length
    part = length // halves
    for i in range(mine.shape[0] // LANES):
        level, step = i // count, i % count
        source = lax.rem(z - step + count, count)
        for ref, flip in ((mine, 0), (sibling, 1)):
            row = (source * count + (f ^ (2 * level) ^ flip)) * LANES
            w[pl.ds(pl.multiple_of(row, LANES), LANES), :] = ref[i * LANES : (i + 1) * LANES, :]
    x[pl.ds(pl.multiple_of(z * length, 64), length), :] = own[...]
    for (offset, valid), a, b in zip(blocks_order, near, far):

        @pl.when(valid(z))
        def _(offset=offset, a=a, b=b):
            at = offset(z) * length
            x[pl.ds(pl.multiple_of(at + t * part, 32), part), :] = a[...]
            x[pl.ds(pl.multiple_of(at + (1 - t) * part, 32), part), :] = b[...]

    half = LANES // 2
    lane = iota((1, LANES), 1)
    first = (lane < half).astype(F32)
    second = 1.0 - first
    ri, ci = iota((LANES, LANES), 0), iota((LANES, LANES), 1)
    same = (ri // half) == (ci // half)
    mean_mat = jnp.where(same, 1.0 / half, 0.0).astype(BF)
    sum_mat = jnp.where(same, 1.0, 0.0).astype(BF)
    strict = same & (ri > ci)
    weak = same & (ri >= ci)
    eye = jnp.where(ri == ci, 1.0, 0.0).astype(F32)

    run = length // 4
    column = pl.ds(pl.multiple_of(z * LANES, LANES), LANES)
    base_row = base[:, column]
    for block in range(count):
        rows = slice(block * length, (block + 1) * length)
        proj[rows, :] = dot_nn(x[rows, :], w[...]).astype(BF)
        decay_in = proj[rows, 3 * LANES : 4 * LANES].astype(F32)
        rate = -jnp.exp(base_row + jnp.tanh(decay_in))
        spare = shards[block, shards.shape[1] - SPARE :, :].astype(F32)
        paces = spare[0:4, :] + spare[4:8, :] + spare[8:12, :]
        for r in range(4):
            log_keep[block * length + r * run : block * length + (r + 1) * run, :] = (
                rate[r * run : (r + 1) * run, :] * paces[r : r + 1, :]
            )

    left = 5 * LANES
    pair = proj[:, left : left + LANES].astype(F32)
    conv_in = (pair * pltpu.roll(sigmoid(pair), half, 1)).astype(BF).astype(F32)
    middle = total_rows // 2
    pad = conv_rows.shape[0] - middle
    moved = pltpu.roll(conv_in[middle - pad :, :], half, 1)
    conv_rows[:pad, :] = moved[:pad, :] * second
    conv_rows[pad:, :] = conv_in[:middle, :] * first + moved[pad:, :] * second
    kernel = taps.shape[0]
    tap = taps[:, pl.ds(pl.multiple_of((z // 2) * LANES, LANES), LANES)]
    turned = pltpu.roll(tap, half, 1)
    odd = (lax.rem(z, 2) == 1).astype(F32)
    tap = jnp.where((lane < half) == (odd < 0.5), tap, turned)
    lead = pad - (kernel - 1)
    strip = 96
    for at in range(0, middle, strip):
        total = jnp.zeros((strip, LANES), F32)
        for j in range(kernel):
            total = total + tap[j : j + 1, :] * conv_rows[at + lead + j : at + lead + j + strip, :]
        total = total.astype(BF)
        out[at : at + strip, LANES : LANES + half] = total[:, :half]
        out[middle + at : middle + at + strip, LANES : LANES + half] = total[:, half:]
    out[:, LANES + half : 2 * LANES] = proj[:, left + LANES : left + LANES + half]

    chunks = total_rows // SPAN
    corr_row = correction[:, column]
    tri = jnp.where(iota((SPAN, SPAN), 0) >= iota((SPAN, SPAN), 1), 1.0, 0.0).astype(F32)

    def stack(a):
        return jnp.concatenate([a * first, a * second], axis=0).astype(BF)

    sums = lax.dot_general(
        tri,
        jnp.concatenate([log_keep[c * SPAN : (c + 1) * SPAN, :] for c in range(chunks)], axis=1),
        (((1,), (0,)), ((), ())),
        precision=lax.Precision.HIGHEST,
        preferred_element_type=F32,
    )
    levels = []
    size = 1
    while size < SPAN:
        inside = (ri // (2 * size)) == (ci // (2 * size))
        levels.append(inside & ((ri & size) != 0) & ((ci & size) == 0))
        size *= 2

    group = 6
    carried = []
    for at in range(0, chunks, group):
        members = list(range(at, min(at + group, chunks)))
        grams, tails, heads = [], [], []
        for c in members:
            rows = slice(c * SPAN, (c + 1) * SPAN)
            total = sums[:, c * LANES : (c + 1) * LANES]
            before = total - log_keep[rows, :]
            last = total[SPAN - 1 : SPAN, :]
            q = proj[rows, 0:LANES].astype(F32)
            k = proj[rows, LANES : 2 * LANES].astype(F32)
            v = proj[rows, 2 * LANES : 3 * LANES].astype(F32)
            norm = dot_nn((k * k).astype(BF), sum_mat)
            unit = k * lax.rsqrt(jnp.maximum(norm, 1.0))
            write = unit * corr_row
            back = jnp.exp(-total)
            rest = jnp.exp(last - total)
            lead_remove = stack(-unit * jnp.exp(before))
            lead_query = stack(q * jnp.exp(total))
            grams.append(
                dot_nt(
                    jnp.concatenate([lead_remove, lead_query], axis=0),
                    jnp.concatenate([stack(write * back), stack(k * back)], axis=0),
                )
            )
            tails.append((stack(write * rest), stack(k * rest), jnp.exp(last)))
            heads.append((lead_remove, lead_query, stack(v)))
        system = [jnp.where(strict, g[:LANES, :LANES], 0.0) for g in grams]
        inverse = [eye + jnp.where(levels[0], a, 0.0) for a in system]
        for level in levels[1:]:
            low = [i.astype(BF) for i in inverse]
            inner = [
                dot_nn(i, jnp.where(level, a, 0.0).astype(BF)).astype(BF) for i, a in zip(low, system)
            ]
            inverse = [i + dot_nn(n, b) for i, n, b in zip(inverse, inner, low)]
        direct = [
            dot_nn(
                jnp.concatenate(
                    [
                        jnp.where(strict, g[:LANES, LANES:], 0.0),
                        jnp.where(weak, g[LANES:, LANES:], 0.0),
                    ],
                    axis=0,
                ).astype(BF),
                h[2],
            )
            for g, h in zip(grams, heads)
        ]
        solved = [
            dot_nn(i.astype(BF), jnp.concatenate([d[:LANES].astype(BF), h[0]], axis=1)).astype(BF)
            for i, d, h in zip(inverse, direct, heads)
        ]
        through = [
            dot_nn(jnp.where(weak, g[LANES:, :LANES], 0.0).astype(BF), s) for g, s in zip(grams, solved)
        ]
        for g, d, s, h, u, tail in zip(grams, direct, solved, heads, through, tails):
            local = u[:, :LANES] + d[LANES:]
            moved = dot_tn(s, tail[0])
            carried.append(
                (
                    local[:SPAN] + local[SPAN:],
                    (h[1].astype(F32) + u[:, LANES:]).astype(BF),
                    moved[LANES:].astype(BF),
                    moved[:LANES] + dot_tn(h[2], tail[1]),
                    tail[2],
                )
            )
    zero = jnp.zeros((half, half), F32)
    state = jnp.concatenate(
        [
            jnp.concatenate([start[2 * z], zero], axis=1),
            jnp.concatenate([zero, start[2 * z + 1]], axis=1),
        ],
        axis=0,
    )
    for c, (local, lead, step, added, kept) in enumerate(carried):
        low = state.astype(BF)
        seen = dot_nt(lead, low)
        y[c * SPAN : (c + 1) * SPAN, :] = local + seen[:SPAN] + seen[SPAN:]
        state = state * kept + dot_nn(low, step) + added

    gain_row = group_gain[:, column]
    for block in range(count):
        rows = slice(block * length, (block + 1) * length)
        values = y[rows, :]
        high = values.astype(BF)
        low = (values - high.astype(F32)).astype(BF)
        centered = values - (dot_nn(high, mean_mat) + dot_nn(low, mean_mat))
        variance = dot_nn((centered * centered).astype(BF), mean_mat)
        gate = proj[rows, 4 * LANES : 5 * LANES].astype(F32)
        grouped = centered * lax.rsqrt(variance + GROUP_FLOOR) * gain_row
        out[rows, :LANES] = (grouped * (gate * sigmoid(gate))).astype(BF)


def output_kernel(place, received, point, *refs, groups):
    pieces, (out, w) = refs[:-2], refs[-2:]
    z, f, t = place[0], place[1], place[2]
    sources, rows, _ = received.shape
    count = sources // groups
    half = LANES // 2
    split = count * half
    wide = count * LANES
    gains = []
    for at, piece in enumerate(pieces):
        core, flip, side = at & 1, (at >> 1) & 1, (at >> 2) & 1
        group = t ^ side
        for block in range(count):
            col = pl.multiple_of((block * count + (f ^ (2 * flip) ^ core)) * LANES, LANES)
            for start, size, shift in (
                (0, split, group * split),
                (split, wide, groups * split + group * wide),
            ):
                w[pl.ds(pl.multiple_of(shift, LANES), size), pl.ds(col, LANES)] = piece[
                    block, start : start + size, :
                ]
        if core == flip == 0:
            spare = piece[0, split + wide :, :].astype(F32)
            tall = split // LANES
            parts = [spare[12 + i * tall : 12 + (i + 1) * tall, :] for i in range(3)]
            total = parts[0] + parts[1] + parts[2]
            gains.append(jnp.concatenate([total[i : i + 1] for i in range(tall)], axis=1))
    gain = jnp.concatenate(
        [jnp.where(t == 0, gains[0], gains[1]), jnp.where(t == 0, gains[1], gains[0])], axis=1
    )
    sums, gates, states = [], [], []
    for group in range(groups):
        for block in range(count):
            source = received[block * groups + group]
            states.append(source[:, :LANES])
            sums.append(source[:, LANES : LANES + half])
            gates.append(source[:, LANES + half :])
    conv_sum = jnp.concatenate(sums, axis=1).astype(F32)
    gate = jnp.concatenate(gates, axis=1).astype(F32)
    mean = jnp.mean(conv_sum, axis=1, keepdims=True)
    spread = jnp.mean(conv_sum * conv_sum, axis=1, keepdims=True) - mean * mean
    scaled = (conv_sum - mean) * lax.rsqrt(spread + CHANNEL_FLOOR) * gain
    shaped = (scaled * sigmoid(scaled)).astype(BF)
    conv_out = (dot_nn(shaped, point[...]) * (gate * sigmoid(gate))).astype(BF)
    joined = jnp.concatenate([conv_out] + states, axis=1)
    out[...] = dot_nn(joined, w[...]).astype(BF)


def ordered_kernel(place, *refs, blocks_order):
    own, *sources, out = refs
    z = place[0]
    out[z] = own[...]
    for (offset, valid), source in zip(blocks_order, sources):

        @pl.when(valid(z))
        def _(offset=offset, source=source):
            out[offset(z)] = source[...]


LINE = (
    ((0, 1), (1, 2), (2, 3)),
    ((1, 0), (2, 1), (3, 2)),
    ((0, 2), (1, 3), (2, 0), (3, 1)),
    ((2, 3), (1, 0)),
)
LINE_ORDER = (
    (lambda z: jnp.maximum(z - 1, 0), lambda z: z > 0),
    (lambda z: jnp.minimum(z + 1, 3), lambda z: z < 3),
    (lambda z: z ^ 2, lambda z: z >= 0),
    (lambda z: z ^ 3, lambda z: (z == 0) | (z == 3)),
)


def along_line(value):
    right, left, double = (lax.ppermute(value, "sp", LINE[i]) for i in range(3))
    return right, left, double, lax.ppermute(double, "sp", LINE[3])


def across(value, pairs):
    targets = sorted({b for _, b in pairs})
    return lax.ppermute(
        value, ("sp", "tp"), [(2 * i + s, 2 * i + 1 - s) for i in targets for s in (0, 1)]
    )


def flipped(value, axis, bit):
    count = lax.axis_size(axis)
    return lax.ppermute(value, axis, [(i, i ^ bit) for i in range(count)])


def head_body(
    tokens, decay_pace, start_state, norm_gain, conv_value, conv_admit, conv_gate, state_query,
    state_key, state_value, state_decay, state_gate, conv_taps, conv_gain, point_weight, decay_base,
    correction, group_gain, output_conv, output_state,
):
    width = tokens.shape[-1]
    length = tokens.shape[1]
    count, halves = lax.axis_size("sp"), lax.axis_size("tp")
    part = length // halves
    place = jnp.stack([lax.axis_index(a) for a in ("sp", "fs", "tp")]).astype(jnp.int32)
    shard = conv_value.shape[0]
    columns = 7 * LANES
    slices = pl.pallas_call(
        split_weights_kernel,
        out_shape=[jax.ShapeDtypeStruct((shard, columns), BF)] * count,
        in_specs=[SM] + [VM] * 8,
        out_specs=[VM] * count,
        name="split_weights",
    )(place, conv_value, conv_admit, conv_gate, state_query, state_key, state_value, state_decay, state_gate)
    taken = [slices[0]] + [
        lax.ppermute(slices[k], "sp", [(s, (s + k) % count) for s in range(count)])
        for k in range(1, count)
    ]
    out_rows = output_conv.shape[0] + output_state.shape[0]
    normed, half, rows_out = pl.pallas_call(
        norm_kernel,
        out_shape=[
            jax.ShapeDtypeStruct((length, width), BF),
            jax.ShapeDtypeStruct((part, width), BF),
            jax.ShapeDtypeStruct((out_rows + SPARE, output_conv.shape[1]), BF),
        ],
        in_specs=[SM] + [VM] * 6,
        out_specs=[VM] * 3,
        name="norm",
    )(
        place[2:], tokens.reshape(length, width), norm_gain.reshape(1, width), output_conv,
        output_state, decay_pace, conv_gain.reshape(1, -1),
    )
    rows_out, _ = lax.optimization_barrier((rows_out, taken[1]))
    line_out = along_line(rows_out)
    half, _ = lax.optimization_barrier((half, line_out[2]))
    near = along_line(half)
    far = [across(a, LINE[i]) for i, a in enumerate(near)]
    lifted = [flipped(a, "fs", 2) for a in taken]
    mine = assemble(*taken, *lifted)
    sibling = flipped(mine, "fs", 1)
    ordered = pl.pallas_call(
        functools.partial(ordered_kernel, blocks_order=LINE_ORDER),
        out_shape=jax.ShapeDtypeStruct((count,) + rows_out.shape, BF),
        in_specs=[SM] + [VM] * 5,
        out_specs=VM,
        name="ordered",
    )(place, rows_out, *line_out)
    crossed = flipped(ordered, "tp", 1)
    pieces = []
    for a in (ordered, crossed):
        for b in (a, flipped(a, "fs", 2)):
            pieces += [b, flipped(b, "fs", 1)]
    total = length * count
    rows = total // (count * halves)
    heads = start_state.shape[1]
    mixed = pl.pallas_call(
        functools.partial(mixer_kernel, length=length, halves=halves, blocks_order=LINE_ORDER),
        out_shape=jax.ShapeDtypeStruct((total, 2 * LANES), BF),
        in_specs=[SM] + [VM] * 17,
        out_specs=VM,
        scratch_shapes=[
            pltpu.VMEM((total, width), BF),
            pltpu.VMEM((width, columns), BF),
            pltpu.VMEM((total, columns), BF),
            pltpu.VMEM((total, LANES), F32),
            pltpu.VMEM((total // 2 + 32, LANES), F32),
            pltpu.VMEM((total, LANES), F32),
        ],
        name="mixer",
    )(
        place, normed, *near, *far, mine, sibling, ordered,
        start_state.reshape(heads, *start_state.shape[2:]),
        decay_base.reshape(1, -1), correction.reshape(1, -1), group_gain.reshape(1, -1), conv_taps,
    )
    received = lax.all_to_all(
        mixed.reshape(count * halves, rows, 2 * LANES), ("sp", "tp"), 0, 0, tiled=True
    )
    out = pl.pallas_call(
        functools.partial(output_kernel, groups=halves),
        out_shape=jax.ShapeDtypeStruct((rows, width), BF),
        in_specs=[SM] + [VM] * 10,
        out_specs=VM,
        scratch_shapes=[pltpu.VMEM((halves * out_rows, width), BF)],
        name="output",
    )(place, received, point_weight, *pieces)
    return out.reshape(1, rows, width)


def passed_along(value, axis, steps):
    count = lax.axis_size(axis)
    leading, last = (max(0, -steps), min(count, count - steps))
    return lax.ppermute(value, axis, [(source, source + steps) for source in range(leading, last)])


def entering_2(value, axis, join, neutral):
    place = lax.axis_index(axis)
    gathered = jax.tree.map(
        lambda a, kind: lax.all_gather(a.astype(kind), axis),
        value,
        jax.tree.map(lambda a: jnp.bfloat16 if a.dtype == jnp.float32 else a.dtype, value),
    )
    state = jax.tree.map(lambda a, e: jnp.zeros_like(a) + jnp.asarray(e, a.dtype), value, neutral)

    def one(lap, state):
        return join(
            state,
            jax.tree.map(
                lambda a, own: lax.dynamic_index_in_dim(a, lap, 0, False).astype(own.dtype),
                gathered,
                value,
            ),
        )

    return lax.fori_loop(0, place, one, state)


def apply_map(matrix, right):
    return jnp.einsum("hbti,hbic->hbtc", matrix, right, precision=lax.Precision.HIGHEST)


def pair_terms(left, right, mask):
    return jnp.einsum("hbtc,hbic->hbti", left, right, precision=lax.Precision.HIGHEST) * mask


def compose(earlier, later):
    first = jnp.matmul(earlier[0], later[0], precision=lax.Precision.HIGHEST)
    second = jnp.matmul(earlier[1], later[0], precision=lax.Precision.HIGHEST) + later[1]
    return (first, second)


def block_terms(query, keys, values, unit, write, log_keep):
    size = query.shape[-1]
    span = query.shape[2]
    total_log = jnp.cumsum(log_keep, axis=2)
    before_log = total_log - log_keep
    last_log = total_log[:, :, span - 1 :, :]
    lead_remove = -unit * jnp.exp(before_log)
    lead_query = query * jnp.exp(total_log)
    back_write = write * jnp.exp(-total_log)
    back_key = keys * jnp.exp(-total_log)
    places = jnp.arange(span)
    strict = (places[:, None] > places[None, :]).astype(jnp.float32)
    weak = (places[:, None] >= places[None, :]).astype(jnp.float32)
    remove_write = pair_terms(lead_remove, back_write, strict)
    remove_key = pair_terms(lead_remove, back_key, strict)
    query_write = pair_terms(lead_query, back_write, weak)
    query_key = pair_terms(lead_query, back_key, weak)
    right_side = jnp.concatenate([apply_map(remove_key, values), lead_remove], axis=-1)
    system = jnp.eye(span, dtype=jnp.float32) - remove_write
    solved = jax.scipy.linalg.solve_triangular(system, right_side, lower=True, unit_diagonal=True)
    own_part = solved[..., :size]
    start_part = solved[..., size:]
    local_out = apply_map(query_write, own_part) + apply_map(query_key, values)
    start_map = lead_query + apply_map(query_write, start_part)
    tail_write = write * jnp.exp(last_log - total_log)
    tail_key = keys * jnp.exp(last_log - total_log)
    carry_map = jnp.einsum(
        "hbtk,hbtj->hbkj", start_part, tail_write, precision=lax.Precision.HIGHEST
    ) + jnp.eye(size, dtype=jnp.float32) * jnp.exp(last_log)
    carry_add = jnp.einsum(
        "hbtv,hbtj->hbvj", own_part, tail_write, precision=lax.Precision.HIGHEST
    ) + jnp.einsum("hbtv,hbtj->hbvj", values, tail_key, precision=lax.Precision.HIGHEST)
    return (local_out, start_map, carry_map, carry_add)


def body(
    tokens,
    decay_pace,
    start_state,
    norm_gain,
    conv_value,
    conv_admit,
    conv_gate,
    state_query,
    state_key,
    state_value,
    state_decay,
    state_gate,
    conv_taps,
    conv_gain,
    point_weight,
    decay_base,
    correction,
    group_gain,
    output_conv,
    output_state,
):
    width = tokens.shape[-1]
    rows = tokens.reshape(-1, width)
    length = rows.shape[0]
    floats = rows.astype(jnp.float32)
    inverse = lax.rsqrt(jnp.mean(floats * floats, axis=1, keepdims=True) + NORM_FLOOR)
    normed = (floats * inverse * norm_gain).astype(jnp.bfloat16)
    shards = (
        conv_value,
        conv_admit,
        conv_gate,
        state_query,
        state_key,
        state_value,
        state_decay,
        state_gate,
    )
    stacked = jnp.concatenate(shards, axis=1)
    projected = jnp.dot(
        normed,
        lax.all_gather(stacked, ("sp", "fs"), axis=0, tiled=True),
        preferred_element_type=jnp.float32,
    ).astype(jnp.bfloat16)
    pieces = []
    offset = 0
    for shard in shards:
        pieces.append(projected[:, offset : offset + shard.shape[1]].astype(jnp.float32))
        offset = offset + shard.shape[1]
    value, admit, gate_conv, query, keys, values, decay_in, gate_state = pieces
    channels = value.shape[1]
    kernel = conv_taps.shape[0]
    conv_input = (value * jax.nn.sigmoid(admit)).astype(jnp.bfloat16)
    earlier = passed_along(conv_input[length - (kernel - 1) :], "sp", 1)
    padded = jnp.concatenate([earlier, conv_input], axis=0).astype(jnp.float32)
    conv_sum = jnp.zeros((length, channels), jnp.float32)
    for place in range(kernel):
        conv_sum = conv_sum + conv_taps[place] * padded[place : place + length]
    local_point = lax.dynamic_slice_in_dim(
        point_weight, lax.axis_index("tp") * channels, channels, 1
    )
    whole_sum, whole_gain = (
        lax.all_gather(conv_sum.astype(jnp.bfloat16), "tp", axis=1, tiled=True).astype(
            conv_sum.dtype
        ),
        lax.all_gather(conv_gain.astype(jnp.bfloat16), "tp", axis=0, tiled=True).astype(
            conv_gain.dtype
        ),
    )
    mean = jnp.mean(whole_sum, axis=1, keepdims=True)
    spread = jnp.mean(whole_sum * whole_sum, axis=1, keepdims=True) - mean * mean
    shaped = jax.nn.silu(
        (whole_sum - mean) * lax.rsqrt(spread + CHANNEL_FLOOR) * whole_gain
    ).astype(jnp.bfloat16)
    pointwise = jnp.dot(shaped, local_point, preferred_element_type=jnp.float32)
    conv_out = (pointwise * jax.nn.silu(gate_conv)).astype(jnp.bfloat16)
    size = start_state.shape[-1]
    heads = query.shape[1] // size
    span = min(64, length)
    blocks = length // span
    log_keep = -jnp.exp(decay_base + jnp.tanh(decay_in)) * decay_pace.reshape(-1)[:, None]
    key_heads = keys.reshape(length, heads, size)
    unit = key_heads * lax.rsqrt(
        jnp.maximum(jnp.sum(key_heads * key_heads, axis=-1, keepdims=True), 1.0)
    )
    write = unit * correction.reshape(heads, size)

    def arrange(array):
        return array.reshape(blocks, span, heads, size).transpose(2, 0, 1, 3)

    local_out, start_map, carry_map, carry_add = block_terms(
        arrange(query),
        arrange(keys),
        arrange(values),
        arrange(unit),
        arrange(write),
        arrange(log_keep),
    )
    identity = (
        jnp.broadcast_to(jnp.eye(size, dtype=jnp.float32), (heads, size, size)),
        jnp.zeros((heads, size, size), jnp.float32),
    )

    def along(carried, block_pair):
        return (compose(carried, block_pair), carried)

    device_pair, prefixes = lax.scan(
        along, identity, (jnp.moveaxis(carry_map, 1, 0), jnp.moveaxis(carry_add, 1, 0))
    )
    prior_map, prior_add = entering_2(device_pair, "sp", compose, identity)
    begin = start_state.reshape(heads, size, size)
    entering = jnp.matmul(begin, prior_map, precision=lax.Precision.HIGHEST) + prior_add
    block_starts = (
        jnp.matmul(entering[None], prefixes[0], precision=lax.Precision.HIGHEST) + prefixes[1]
    )
    block_starts = jnp.moveaxis(block_starts, 0, 1)
    outputs = local_out + jnp.einsum(
        "hbtk,hbvk->hbtv", start_map, block_starts, precision=lax.Precision.HIGHEST
    )
    outputs = outputs.transpose(1, 2, 0, 3).reshape(length, heads, size)
    centered = outputs - jnp.mean(outputs, axis=-1, keepdims=True)
    variance = jnp.mean(centered * centered, axis=-1, keepdims=True)
    grouped = centered * lax.rsqrt(variance + GROUP_FLOOR) * group_gain.reshape(heads, size)
    state_out = (grouped.reshape(length, heads * size) * jax.nn.silu(gate_state)).astype(
        jnp.bfloat16
    )
    local_mix = jnp.concatenate([conv_out, state_out], axis=1)
    moved = lax.all_to_all(local_mix, "tp", split_axis=0, concat_axis=1, tiled=True)
    conv_rows, state_rows = (
        lax.all_gather(output_conv, "tp", axis=0, tiled=True),
        lax.all_gather(output_state, "tp", axis=0, tiled=True),
    )
    groups = lax.axis_size("tp")
    joined = jnp.concatenate(
        [conv_rows.reshape(groups, channels, -1), state_rows.reshape(groups, heads * size, -1)],
        axis=1,
    )
    joined = joined.reshape(groups * (channels + heads * size), -1)
    mixed = jnp.dot(
        moved,
        lax.all_gather(joined, ("sp", "fs"), axis=1, tiled=True),
        preferred_element_type=jnp.float32,
    )
    return mixed.astype(jnp.bfloat16).reshape(1, -1, width)


def layer(*args):
    sizes = [lax.axis_size(a) for a in ("sp", "fs", "tp")]
    channels, wide = args[4].shape[1], args[7].shape[1]
    whole = channels == sizes[0] * LANES // 2 and wide == sizes[0] * LANES
    square = args[2].shape[-1] == LANES // 2 and args[4].shape[0] == LANES
    return (head_body if sizes == [4, 4, 2] and whole and square else body)(*args)


def solution(mesh):
    return jax.shard_map(
        layer,
        mesh=mesh,
        in_specs=(
            P("fs", "sp", None),
            P("fs", "sp"),
            P("fs", "tp", None, None),
            P(),
            P(("sp", "fs"), "tp"),
            P(("sp", "fs"), "tp"),
            P(("sp", "fs"), "tp"),
            P(("sp", "fs"), "tp"),
            P(("sp", "fs"), "tp"),
            P(("sp", "fs"), "tp"),
            P(("sp", "fs"), "tp"),
            P(("sp", "fs"), "tp"),
            P(None, "tp"),
            P("tp"),
            P(),
            P("tp"),
            P("tp"),
            P("tp"),
            P("tp", ("sp", "fs")),
            P("tp", ("sp", "fs")),
        ),
        out_specs=P("fs", ("sp", "tp"), None),
        check_vma=False,
    )
```

```python
import functools

import jax
import jax.numpy as jnp
from jax import lax
from jax.experimental import pallas as pl
from jax.experimental.pallas import tpu as pltpu
from jax.sharding import PartitionSpec as P

NORM_FLOOR = 0.1
CHANNEL_FLOOR = 0.1
GROUP_FLOOR = 1.0
LANES = 128
SPAN = 64
SPARE = 16
BF = jnp.bfloat16
F32 = jnp.float32
VM = pl.BlockSpec(memory_space=pltpu.VMEM)


def dot_nn(a, b):
    return lax.dot_general(a, b, (((1,), (0,)), ((), ())), preferred_element_type=F32)


def dot_nt(a, b):
    return lax.dot_general(a, b, (((1,), (1,)), ((), ())), preferred_element_type=F32)


def dot_tn(a, b):
    return lax.dot_general(a, b, (((0,), (0,)), ((), ())), preferred_element_type=F32)


def sigmoid(x):
    return 1.0 / (1.0 + jnp.exp(-x))


def iota(shape, dim):
    return lax.broadcasted_iota(jnp.int32, shape, dim)


def three_terms(a):
    high = a.astype(BF).astype(F32)
    middle = (a - high).astype(BF).astype(F32)
    return high, middle, a - high - middle


def here():
    return [lax.axis_index(a) for a in ("sp", "fs", "tp")]


def split_weights_kernel(*refs):
    pace, convs, states, outs = refs[0], refs[1:4], refs[4:9], refs[9:]
    run = pace.shape[1] // 4
    paces = jnp.concatenate(
        [jnp.broadcast_to(pace[:, r * run : r * run + 1], (1, LANES // 2)) for r in range(4)], axis=0
    )
    rest = jnp.zeros((convs[0].shape[0] - 12, LANES // 2), F32)
    spare = jnp.concatenate([*three_terms(paces), rest], axis=0).astype(BF)
    half = LANES // 2
    z = here()[0]
    for step, out in enumerate(outs):
        target = z ^ step
        for at, ref in enumerate(states):
            out[:, at * LANES : (at + 1) * LANES] = ref[
                :, pl.ds(pl.multiple_of(target * LANES, LANES), LANES)
            ]
        odd = lax.rem(target, 2) == 1
        for at, ref in enumerate(convs):
            pair = ref[:, pl.ds(pl.multiple_of((target // 2) * LANES, LANES), LANES)]
            start = len(states) * LANES + at * half
            out[:, start : start + half] = jnp.where(odd, pair[:, half:], pair[:, :half])
        out[:, start + half :] = spare


def norm_kernel(tokens, gain, out_conv, out_state, conv_gain, normed, part, rows_out):
    count = part.shape[0]
    floats = tokens[...].astype(F32)
    inverse = lax.rsqrt(jnp.mean(floats * floats, axis=1, keepdims=True) + NORM_FLOOR)
    normed[...] = (floats * inverse * gain[...]).astype(BF)
    part[...] = normed[pl.ds(pl.multiple_of(here()[2] * count, 16), count), :]
    split, wide = out_conv.shape[0], out_state.shape[0]
    rows_out[:split, :] = out_conv[...]
    rows_out[split : split + wide, :] = out_state[...]
    gains = jnp.concatenate(
        [conv_gain[:, i * LANES : (i + 1) * LANES] for i in range(split // LANES)], axis=0
    )
    spare = jnp.concatenate(
        list(three_terms(gains)) + [jnp.zeros((SPARE - 3 * gains.shape[0], LANES), F32)],
        axis=0,
    )
    rows_out[split + wide :, :] = spare.astype(BF)


def assemble_kernel(*refs):
    *sources, out = refs
    size = sources[0].shape[0]
    for i, source in enumerate(sources):
        out[i * size : (i + 1) * size, :] = source[...]


def call(kernel, outs, *args, scratch=(), held=(), whole=(), room=10, **settings):
    specs, operands = [], []
    for at, arg in enumerate(args):
        specs.append(pl.BlockSpec(memory_space=pl.ANY) if at in whole else VM)
        apart = at in held or at in whole
        operands.append(pltpu.with_memory_space_constraint(arg, pltpu.HBM if apart else pltpu.VMEM))
    return pl.pallas_call(
        functools.partial(kernel, **settings) if settings else kernel,
        out_shape=[pltpu.VMEM(*o) if isinstance(o, tuple) else o for o in outs],
        in_specs=specs,
        out_specs=[VM] * len(outs),
        scratch_shapes=[pltpu.VMEM(*a) if isinstance(a, tuple) else a for a in scratch],
        compiler_params=pltpu.CompilerParams(vmem_limit_bytes=room << 20),
    )(*operands)


def masks():
    half = LANES // 2
    lane = iota((1, LANES), 1)
    first = (lane < half).astype(F32)
    ri, ci = iota((LANES, LANES), 0), iota((LANES, LANES), 1)
    return first, 1.0 - first, ri, ci, (ri // half) == (ci // half)


def stage_terms(x, w, paces, base_row, corr_row, conv_part, gate_part, local, lead, step, added, kept, proj, log_keep):
    length = x.shape[0]
    first, second, ri, ci, same = masks()
    sum_mat = jnp.where(same, 1.0, 0.0).astype(BF)
    strict = same & (ri > ci)
    weak = same & (ri >= ci)
    eye = jnp.where(ri == ci, 1.0, 0.0).astype(F32)
    run = length // 4
    proj[...] = dot_nn(x[...], w[...])
    gate_part[...] = proj[:, 4 * LANES : 5 * LANES].astype(BF)
    conv_part[...] = proj[:, 5 * LANES : 7 * LANES].astype(BF)
    rate = -jnp.exp(base_row + jnp.tanh(proj[:, 3 * LANES : 4 * LANES].astype(BF).astype(F32)))
    for r in range(4):
        log_keep[r * run : (r + 1) * run, :] = rate[r * run : (r + 1) * run, :] * paces[r : r + 1, :]

    chunks = length // SPAN
    tri = jnp.where(iota((SPAN, SPAN), 0) >= iota((SPAN, SPAN), 1), 1.0, 0.0).astype(F32)

    def stack(a):
        return jnp.concatenate([a * first, a * second], axis=0).astype(BF)

    sums = lax.dot_general(
        tri,
        jnp.concatenate([log_keep[c * SPAN : (c + 1) * SPAN, :] for c in range(chunks)], axis=1),
        (((1,), (0,)), ((), ())),
        precision=lax.Precision.HIGHEST,
        preferred_element_type=F32,
    )
    levels = []
    size = 1
    while size < SPAN:
        inside = (ri // (2 * size)) == (ci // (2 * size))
        levels.append(inside & ((ri & size) != 0) & ((ci & size) == 0))
        size *= 2
    grams, tails, heads = [], [], []
    for c in range(chunks):
        rows = slice(c * SPAN, (c + 1) * SPAN)
        total = sums[:, c * LANES : (c + 1) * LANES]
        before = total - log_keep[rows, :]
        last = total[SPAN - 1 : SPAN, :]
        q = proj[rows, 0:LANES].astype(BF).astype(F32)
        k = proj[rows, LANES : 2 * LANES].astype(BF).astype(F32)
        v = proj[rows, 2 * LANES : 3 * LANES]
        norm = dot_nn((k * k).astype(BF), sum_mat)
        unit = k * lax.rsqrt(jnp.maximum(norm, 1.0))
        write = unit * corr_row
        back = jnp.exp(-total)
        rest = jnp.exp(last - total)
        lead_remove = stack(-unit * jnp.exp(before))
        lead_query = stack(q * jnp.exp(total))
        grams.append(
            dot_nt(
                jnp.concatenate([lead_remove, lead_query], axis=0),
                jnp.concatenate([stack(write * back), stack(k * back)], axis=0),
            )
        )
        tails.append((stack(write * rest), stack(k * rest)))
        heads.append((lead_remove, lead_query, stack(v)))
        kept[c] = jnp.broadcast_to(jnp.exp(last), kept.shape[1:])
    system = [jnp.where(strict, g[:LANES, :LANES], 0.0) for g in grams]
    inverse = [eye + jnp.where(levels[0], a, 0.0) for a in system]
    for level in levels[1:]:
        low = [i.astype(BF) for i in inverse]
        inner = [
            dot_nn(i, jnp.where(level, a, 0.0).astype(BF)).astype(BF) for i, a in zip(low, system)
        ]
        inverse = [i + dot_nn(n, b) for i, n, b in zip(inverse, inner, low)]
    direct = [
        dot_nn(
            jnp.concatenate(
                [
                    jnp.where(strict, g[:LANES, LANES:], 0.0),
                    jnp.where(weak, g[LANES:, LANES:], 0.0),
                ],
                axis=0,
            ).astype(BF),
            h[2],
        )
        for g, h in zip(grams, heads)
    ]
    solved = [
        dot_nn(i.astype(BF), jnp.concatenate([d[:LANES].astype(BF), h[0]], axis=1)).astype(BF)
        for i, d, h in zip(inverse, direct, heads)
    ]
    through = [
        dot_nn(jnp.where(weak, g[LANES:, :LANES], 0.0).astype(BF), s) for g, s in zip(grams, solved)
    ]
    for c, (d, s, h, u, tail) in enumerate(zip(direct, solved, heads, through, tails)):
        own = u[:, :LANES] + d[LANES:]
        moved = dot_tn(s, tail[0])
        local[c] = own[:SPAN] + own[SPAN:]
        lead[c] = (h[1].astype(F32) + u[:, LANES:]).astype(BF)
        step[c] = moved[LANES:].astype(BF)
        added[c] = moved[:LANES] + dot_tn(h[2], tail[1])


def own_kernel(x, mine, sibling, base, correction, w, *outs):
    z, f, _ = here()
    count = lax.axis_size("sp")
    for i in range(mine.shape[0] // LANES):
        level, step = i // count, i % count
        source = z ^ step
        for ref, flip in ((mine, 0), (sibling, 1)):
            row = (source * lax.axis_size("fs") + (f ^ (2 * level) ^ flip)) * LANES
            w[pl.ds(pl.multiple_of(row, LANES), LANES), :] = ref[i * LANES : (i + 1) * LANES, :]
    block_terms_in(z, x, w, base, correction, outs)


def block_terms_in(position, x, w, base, correction, refs):
    row = (position * lax.axis_size("fs") + here()[1]) * LANES
    spare = w[pl.ds(pl.multiple_of(row, LANES), 16), w.shape[1] - LANES :].astype(F32)
    paces = spare[0:4, :] + spare[4:8, :] + spare[8:12, :]
    paces = jnp.concatenate([paces[:, LANES // 2 :]] * 2, axis=1)
    stage_terms(x, w, paces, base[...], correction[...], *refs)


def prepare_kernel(start, base, correction, group_gain, taps, state, *outs):
    z = here()[0]
    half = LANES // 2
    column = pl.ds(pl.multiple_of(z * LANES, LANES), LANES)
    *rows, tap_rows = outs
    for row, ref in zip(rows, (base, correction, group_gain)):
        row[...] = ref[:, column]
    zero = jnp.zeros((half, half), F32)
    state[:half, :] = jnp.concatenate([start[2 * z], zero], axis=1)
    state[half:, :] = jnp.concatenate([zero, start[2 * z + 1]], axis=1)
    tap = taps[:, pl.ds(pl.multiple_of((z // 2) * LANES, LANES), LANES)]
    tap_rows[: taps.shape[0], :] = tap


def block_kernel(*refs, step, conditions):
    count = len(conditions)
    sources = refs[: 2 * count]
    w, base, correction = refs[2 * count : 2 * count + 3]
    *outs, proj, log_keep, x = refs[2 * count + 3 :]
    z, _, t = here()
    part = x.shape[0] // 2
    for at, holds in enumerate(conditions):
        a, b = sources[2 * at : 2 * at + 2]

        def put(a=a, b=b):
            x[pl.ds(pl.multiple_of(t * part, 32), part), :] = a[...]
            x[pl.ds(pl.multiple_of((1 - t) * part, 32), part), :] = b[...]

        put() if holds is None else pl.when(holds(z))(put)
    block_terms_in(z ^ step, x, w, base, correction, (*outs, proj, log_keep))


def final_kernel(*refs, count, width):
    slots = [refs[7 * i : 7 * (i + 1)] for i in range(count)]
    start, rows_in, tap, out, conv, gates, local, lead, step, added, kept, conv_rows, y = refs[
        7 * count :
    ]
    z = here()[0]
    half = LANES // 2
    first, second, _, _, same = masks()
    mean_mat = jnp.where(same, 1.0 / half, 0.0).astype(BF)
    length = conv.shape[1]
    total_rows = count * length
    for at, slot in enumerate(slots):
        position = z ^ at
        for target, source in zip((conv, gates, local, lead, step, added, kept), slot):
            target[position] = source[...]

    middle = total_rows // 2
    pad = conv_rows.shape[0] - middle
    for block in range(count):
        pair = conv[block, :, :LANES].astype(F32)
        conv_in = (pair * pltpu.roll(sigmoid(pair), half, 1)).astype(BF).astype(F32)
        at = block * length
        if at < middle:
            conv_rows[pad + at : pad + at + length, :] = conv_in * first
            if at + length == middle:
                conv_rows[:pad, :] = pltpu.roll(conv_in[length - pad :, :], half, 1) * second
        else:
            rows = slice(pad + at - middle, pad + at - middle + length)
            conv_rows[rows, :] = conv_rows[rows, :] + pltpu.roll(conv_in, half, 1) * second
        out[at : at + length, LANES + half : 2 * LANES] = conv[block, :, LANES : LANES + half]
    tap = tap[:width, :]
    odd = (lax.rem(z, 2) == 1).astype(F32)
    left = iota((1, LANES), 1) < half
    tap = jnp.where(left == (odd < 0.5), tap, pltpu.roll(tap, half, 1))
    shift = pad - (width - 1)
    strip = 96
    for at in range(0, middle, strip):
        total = jnp.zeros((strip, LANES), F32)
        for j in range(width):
            total = total + tap[j : j + 1, :] * conv_rows[at + shift + j : at + shift + j + strip, :]
        total = total.astype(BF)
        out[at : at + strip, LANES : LANES + half] = total[:, :half]
        out[middle + at : middle + at + strip, LANES : LANES + half] = total[:, half:]

    state = start[...]
    chunks = length // SPAN
    for c in range(count * chunks):
        at = (c // chunks, c % chunks)
        low = state.astype(BF)
        seen = dot_nt(lead[at], low)
        y[c * SPAN : (c + 1) * SPAN, :] = local[at] + seen[:SPAN] + seen[SPAN:]
        state = state * kept[at][:1] + dot_nn(low, step[at]) + added[at]

    gain_row = rows_in[...]
    for block in range(count):
        rows = slice(block * length, (block + 1) * length)
        values = y[rows, :]
        high = values.astype(BF)
        low = (values - high.astype(F32)).astype(BF)
        centered = values - (dot_nn(high, mean_mat) + dot_nn(low, mean_mat))
        variance = dot_nn((centered * centered).astype(BF), mean_mat)
        gate = gates[block].astype(F32)
        grouped = centered * lax.rsqrt(variance + GROUP_FLOOR) * gain_row
        out[rows, :LANES] = (grouped * (gate * sigmoid(gate))).astype(BF)


def output_kernel(received, point, *refs, groups):
    *pieces, out, w = refs
    _, f, t = here()
    count = pieces[0].shape[0]
    split = count * LANES // 2
    wide = count * LANES
    gains = []
    for at, piece in enumerate(pieces):
        core, flip, side = at & 1, (at >> 1) & 1, (at >> 2) & 1
        group = t ^ side
        for block in range(count):
            col = pl.multiple_of((block * count + (f ^ (2 * flip) ^ core)) * LANES, LANES)
            for start, size, shift in (
                (0, split, group * split),
                (split, wide, groups * split + group * wide),
            ):
                w[pl.ds(pl.multiple_of(shift, LANES), size), pl.ds(col, LANES)] = piece[
                    block, start : start + size, :
                ]
        if core == flip == 0:
            spare = piece[0, split + wide :, :].astype(F32)
            tall = split // LANES
            parts = [spare[i * tall : (i + 1) * tall, :] for i in range(3)]
            total = parts[0] + parts[1] + parts[2]
            gains.append(jnp.concatenate([total[i : i + 1] for i in range(tall)], axis=1))
    gain = jnp.concatenate(
        [jnp.where(t == 0, gains[0], gains[1]), jnp.where(t == 0, gains[1], gains[0])], axis=1
    )
    half = LANES // 2
    sums, gates, states = [], [], []
    for group in range(groups):
        for block in range(count):
            source = received[block * groups + group]
            states.append(source[:, :LANES])
            sums.append(source[:, LANES : LANES + half])
            gates.append(source[:, LANES + half :])
    conv_sum = jnp.concatenate(sums, axis=1).astype(F32)
    gate = jnp.concatenate(gates, axis=1).astype(F32)
    mean = jnp.mean(conv_sum, axis=1, keepdims=True)
    spread = jnp.mean(conv_sum * conv_sum, axis=1, keepdims=True) - mean * mean
    scaled = (conv_sum - mean) * lax.rsqrt(spread + CHANNEL_FLOOR) * gain
    shaped = (scaled * sigmoid(scaled)).astype(BF)
    conv_out = (dot_nn(shaped, point[...]) * (gate * sigmoid(gate))).astype(BF)
    joined = jnp.concatenate([conv_out] + states, axis=1)
    out[...] = dot_nn(joined, w[...]).astype(BF)


def ordered_kernel(own, *refs):
    *sources, out = refs
    z = here()[0]
    out[z] = own[...]
    for step, choices in ARRIVALS:
        for at, holds in choices:

            def put(step=step, at=at):
                out[z ^ step] = sources[at][...]

            put() if holds is None else pl.when(holds(z))(put)


LINE = (
    ((0, 1), (1, 0), (2, 3), (3, 2)),
    ((0, 2), (1, 3), (2, 0), (3, 1)),
    ((1, 2), (2, 1)),
    ((2, 3), (1, 0)),
)
FORWARD = {3: 1}


def inner(z):
    return (z == 1) | (z == 2)


def outer(z):
    return (z == 0) | (z == 3)


ARRIVALS = (
    (1, ((0, None),)),
    (2, ((1, None),)),
    (3, ((2, inner), (3, outer))),
)


def along_line(value):
    moved = []
    for i, pairs in enumerate(LINE):
        moved.append(lax.ppermute(moved[FORWARD[i]] if i in FORWARD else value, "sp", pairs))
    return moved


def across(value, pairs):
    targets = sorted({b for _, b in pairs})
    return lax.ppermute(
        value, ("sp", "tp"), [(2 * i + s, 2 * i + 1 - s) for i in targets for s in (0, 1)]
    )


def flipped(value, axis, bit):
    count = lax.axis_size(axis)
    return lax.ppermute(value, axis, [(i, i ^ bit) for i in range(count)])


def head_body(
    tokens, decay_pace, start_state, norm_gain, conv_value, conv_admit, conv_gate, state_query,
    state_key, state_value, state_decay, state_gate, conv_taps, conv_gain, point_weight, decay_base,
    correction, group_gain, output_conv, output_state,
):
    width = tokens.shape[-1]
    length = tokens.shape[1]
    count, halves = lax.axis_size("sp"), lax.axis_size("tp")
    part = length // halves
    shard = conv_value.shape[0]
    columns = 7 * LANES
    slices = call(
        split_weights_kernel, [((shard, columns), BF)] * count,
        decay_pace, conv_value, conv_admit, conv_gate, state_query, state_key, state_value, state_decay,
        state_gate, held=range(9),
    )
    taken = [slices[0]] + [flipped(slices[k], "sp", k) for k in range(1, count)]
    out_rows = output_conv.shape[0] + output_state.shape[0]
    normed, half, rows_out = call(
        norm_kernel,
        [pltpu.HBM((length, width), BF), ((part, width), BF), ((out_rows + SPARE, output_conv.shape[1]), BF)],
        tokens.reshape(length, width), norm_gain.reshape(1, width), output_conv,
        output_state, conv_gain.reshape(1, -1), held=range(5),
    )
    line_out = along_line(rows_out)
    near = along_line(half)
    far = [across(a, LINE[i]) for i, a in enumerate(near)]
    lifted = [flipped(a, "fs", 2) for a in taken]
    (mine,) = call(assemble_kernel, [((2 * count * shard, columns), BF)], *taken, *lifted)
    sibling = flipped(mine, "fs", 1)
    (ordered,) = call(ordered_kernel, [((count,) + rows_out.shape, BF)], rows_out, *line_out)
    crossed = flipped(ordered, "tp", 1)
    pieces = []
    for a in (ordered, crossed):
        for b in (a, flipped(a, "fs", 2)):
            pieces += [b, flipped(b, "fs", 1)]
    total = length * count
    rows = total // (count * halves)
    chunks = length // SPAN
    terms = [
        ((length, 2 * LANES), BF),
        ((length, LANES), BF),
        ((chunks, SPAN, LANES), F32),
        ((chunks, LANES, LANES), BF),
        ((chunks, LANES, LANES), BF),
        ((chunks, LANES, LANES), F32),
        ((chunks, 8, LANES), F32),
    ]
    work = [((length, columns), F32), ((length, LANES), F32)]
    heads = start_state.shape[1]
    kernel = conv_taps.shape[0]
    begin, *small, gains, tap = call(
        prepare_kernel,
        [((LANES, LANES), F32)] + [((1, LANES), F32)] * 3 + [((-(-kernel // 8) * 8, LANES), F32)],
        start_state.reshape(heads, *start_state.shape[2:]), decay_base.reshape(1, -1),
        correction.reshape(1, -1), group_gain.reshape(1, -1), conv_taps, held=range(5),
    )
    w, *slots = call(
        own_kernel, [((width, columns), BF)] + terms,
        normed, mine, sibling, *small, held=(0,), scratch=work,
    )
    for step, choices in ARRIVALS:
        sources = [a for i, _ in choices for a in (near[i], far[i])]
        slots += call(
            block_kernel, terms, *sources, w, *small,
            scratch=work + [((length, width), BF)],
            step=step, conditions=tuple(holds for _, holds in choices),
        )
    mixed = call(
        final_kernel, [((total, 2 * LANES), BF)], *slots, begin, gains, tap,
        count=count, width=kernel,
        scratch=[((count,) + a, b) for a, b in terms]
        + [((total // 2 + 32, LANES), F32), ((total, LANES), F32)],
    )[0]
    received = lax.all_to_all(
        mixed.reshape(count * halves, rows, 2 * LANES), ("sp", "tp"), 0, 0, tiled=True
    )
    (out,) = call(
        output_kernel, [jax.ShapeDtypeStruct((rows, width), BF)],
        received, point_weight, *pieces, held=(1,), room=20, groups=halves,
        scratch=[((halves * out_rows, width), BF)],
    )
    return out.reshape(1, rows, width)


def passed_along(value, axis, steps):
    count = lax.axis_size(axis)
    leading, last = (max(0, -steps), min(count, count - steps))
    return lax.ppermute(value, axis, [(source, source + steps) for source in range(leading, last)])


def entering_2(value, axis, join, neutral):
    place = lax.axis_index(axis)
    gathered = jax.tree.map(
        lambda a, kind: lax.all_gather(a.astype(kind), axis),
        value,
        jax.tree.map(lambda a: jnp.bfloat16 if a.dtype == jnp.float32 else a.dtype, value),
    )
    state = jax.tree.map(lambda a, e: jnp.zeros_like(a) + jnp.asarray(e, a.dtype), value, neutral)

    def one(lap, state):
        return join(
            state,
            jax.tree.map(
                lambda a, own: lax.dynamic_index_in_dim(a, lap, 0, False).astype(own.dtype),
                gathered,
                value,
            ),
        )

    return lax.fori_loop(0, place, one, state)


def apply_map(matrix, right):
    return jnp.einsum("hbti,hbic->hbtc", matrix, right, precision=lax.Precision.HIGHEST)


def pair_terms(left, right, mask):
    return jnp.einsum("hbtc,hbic->hbti", left, right, precision=lax.Precision.HIGHEST) * mask


def compose(earlier, later):
    first = jnp.matmul(earlier[0], later[0], precision=lax.Precision.HIGHEST)
    second = jnp.matmul(earlier[1], later[0], precision=lax.Precision.HIGHEST) + later[1]
    return (first, second)


def block_terms(query, keys, values, unit, write, log_keep):
    size = query.shape[-1]
    span = query.shape[2]
    total_log = jnp.cumsum(log_keep, axis=2)
    before_log = total_log - log_keep
    last_log = total_log[:, :, span - 1 :, :]
    lead_remove = -unit * jnp.exp(before_log)
    lead_query = query * jnp.exp(total_log)
    back_write = write * jnp.exp(-total_log)
    back_key = keys * jnp.exp(-total_log)
    places = jnp.arange(span)
    strict = (places[:, None] > places[None, :]).astype(jnp.float32)
    weak = (places[:, None] >= places[None, :]).astype(jnp.float32)
    remove_write = pair_terms(lead_remove, back_write, strict)
    remove_key = pair_terms(lead_remove, back_key, strict)
    query_write = pair_terms(lead_query, back_write, weak)
    query_key = pair_terms(lead_query, back_key, weak)
    right_side = jnp.concatenate([apply_map(remove_key, values), lead_remove], axis=-1)
    system = jnp.eye(span, dtype=jnp.float32) - remove_write
    solved = jax.scipy.linalg.solve_triangular(system, right_side, lower=True, unit_diagonal=True)
    own_part = solved[..., :size]
    start_part = solved[..., size:]
    local_out = apply_map(query_write, own_part) + apply_map(query_key, values)
    start_map = lead_query + apply_map(query_write, start_part)
    tail_write = write * jnp.exp(last_log - total_log)
    tail_key = keys * jnp.exp(last_log - total_log)
    carry_map = jnp.einsum(
        "hbtk,hbtj->hbkj", start_part, tail_write, precision=lax.Precision.HIGHEST
    ) + jnp.eye(size, dtype=jnp.float32) * jnp.exp(last_log)
    carry_add = jnp.einsum(
        "hbtv,hbtj->hbvj", own_part, tail_write, precision=lax.Precision.HIGHEST
    ) + jnp.einsum("hbtv,hbtj->hbvj", values, tail_key, precision=lax.Precision.HIGHEST)
    return (local_out, start_map, carry_map, carry_add)


def body(
    tokens,
    decay_pace,
    start_state,
    norm_gain,
    conv_value,
    conv_admit,
    conv_gate,
    state_query,
    state_key,
    state_value,
    state_decay,
    state_gate,
    conv_taps,
    conv_gain,
    point_weight,
    decay_base,
    correction,
    group_gain,
    output_conv,
    output_state,
):
    width = tokens.shape[-1]
    rows = tokens.reshape(-1, width)
    length = rows.shape[0]
    floats = rows.astype(jnp.float32)
    inverse = lax.rsqrt(jnp.mean(floats * floats, axis=1, keepdims=True) + NORM_FLOOR)
    normed = (floats * inverse * norm_gain).astype(jnp.bfloat16)
    shards = (
        conv_value,
        conv_admit,
        conv_gate,
        state_query,
        state_key,
        state_value,
        state_decay,
        state_gate,
    )
    stacked = jnp.concatenate(shards, axis=1)
    projected = jnp.dot(
        normed,
        lax.all_gather(stacked, ("sp", "fs"), axis=0, tiled=True),
        preferred_element_type=jnp.float32,
    ).astype(jnp.bfloat16)
    pieces = []
    offset = 0
    for shard in shards:
        pieces.append(projected[:, offset : offset + shard.shape[1]].astype(jnp.float32))
        offset = offset + shard.shape[1]
    value, admit, gate_conv, query, keys, values, decay_in, gate_state = pieces
    channels = value.shape[1]
    kernel = conv_taps.shape[0]
    conv_input = (value * jax.nn.sigmoid(admit)).astype(jnp.bfloat16)
    earlier = passed_along(conv_input[length - (kernel - 1) :], "sp", 1)
    padded = jnp.concatenate([earlier, conv_input], axis=0).astype(jnp.float32)
    conv_sum = jnp.zeros((length, channels), jnp.float32)
    for place in range(kernel):
        conv_sum = conv_sum + conv_taps[place] * padded[place : place + length]
    local_point = lax.dynamic_slice_in_dim(
        point_weight, lax.axis_index("tp") * channels, channels, 1
    )
    whole_sum, whole_gain = (
        lax.all_gather(conv_sum.astype(jnp.bfloat16), "tp", axis=1, tiled=True).astype(
            conv_sum.dtype
        ),
        lax.all_gather(conv_gain.astype(jnp.bfloat16), "tp", axis=0, tiled=True).astype(
            conv_gain.dtype
        ),
    )
    mean = jnp.mean(whole_sum, axis=1, keepdims=True)
    spread = jnp.mean(whole_sum * whole_sum, axis=1, keepdims=True) - mean * mean
    shaped = jax.nn.silu(
        (whole_sum - mean) * lax.rsqrt(spread + CHANNEL_FLOOR) * whole_gain
    ).astype(jnp.bfloat16)
    pointwise = jnp.dot(shaped, local_point, preferred_element_type=jnp.float32)
    conv_out = (pointwise * jax.nn.silu(gate_conv)).astype(jnp.bfloat16)
    size = start_state.shape[-1]
    heads = query.shape[1] // size
    span = min(64, length)
    blocks = length // span
    log_keep = -jnp.exp(decay_base + jnp.tanh(decay_in)) * decay_pace.reshape(-1)[:, None]
    key_heads = keys.reshape(length, heads, size)
    unit = key_heads * lax.rsqrt(
        jnp.maximum(jnp.sum(key_heads * key_heads, axis=-1, keepdims=True), 1.0)
    )
    write = unit * correction.reshape(heads, size)

    def arrange(array):
        return array.reshape(blocks, span, heads, size).transpose(2, 0, 1, 3)

    local_out, start_map, carry_map, carry_add = block_terms(
        arrange(query),
        arrange(keys),
        arrange(values),
        arrange(unit),
        arrange(write),
        arrange(log_keep),
    )
    identity = (
        jnp.broadcast_to(jnp.eye(size, dtype=jnp.float32), (heads, size, size)),
        jnp.zeros((heads, size, size), jnp.float32),
    )

    def along(carried, block_pair):
        return (compose(carried, block_pair), carried)

    device_pair, prefixes = lax.scan(
        along, identity, (jnp.moveaxis(carry_map, 1, 0), jnp.moveaxis(carry_add, 1, 0))
    )
    prior_map, prior_add = entering_2(device_pair, "sp", compose, identity)
    begin = start_state.reshape(heads, size, size)
    entering = jnp.matmul(begin, prior_map, precision=lax.Precision.HIGHEST) + prior_add
    block_starts = (
        jnp.matmul(entering[None], prefixes[0], precision=lax.Precision.HIGHEST) + prefixes[1]
    )
    block_starts = jnp.moveaxis(block_starts, 0, 1)
    outputs = local_out + jnp.einsum(
        "hbtk,hbvk->hbtv", start_map, block_starts, precision=lax.Precision.HIGHEST
    )
    outputs = outputs.transpose(1, 2, 0, 3).reshape(length, heads, size)
    centered = outputs - jnp.mean(outputs, axis=-1, keepdims=True)
    variance = jnp.mean(centered * centered, axis=-1, keepdims=True)
    grouped = centered * lax.rsqrt(variance + GROUP_FLOOR) * group_gain.reshape(heads, size)
    state_out = (grouped.reshape(length, heads * size) * jax.nn.silu(gate_state)).astype(
        jnp.bfloat16
    )
    local_mix = jnp.concatenate([conv_out, state_out], axis=1)
    moved = lax.all_to_all(local_mix, "tp", split_axis=0, concat_axis=1, tiled=True)
    conv_rows, state_rows = (
        lax.all_gather(output_conv, "tp", axis=0, tiled=True),
        lax.all_gather(output_state, "tp", axis=0, tiled=True),
    )
    groups = lax.axis_size("tp")
    joined = jnp.concatenate(
        [conv_rows.reshape(groups, channels, -1), state_rows.reshape(groups, heads * size, -1)],
        axis=1,
    )
    joined = joined.reshape(groups * (channels + heads * size), -1)
    mixed = jnp.dot(
        moved,
        lax.all_gather(joined, ("sp", "fs"), axis=1, tiled=True),
        preferred_element_type=jnp.float32,
    )
    return mixed.astype(jnp.bfloat16).reshape(1, -1, width)


def layer(*args):
    sizes = [lax.axis_size(a) for a in ("sp", "fs", "tp")]
    channels, wide = args[4].shape[1], args[7].shape[1]
    whole = channels == sizes[0] * LANES // 2 and wide == sizes[0] * LANES
    square = args[2].shape[-1] == LANES // 2 and args[4].shape[0] == LANES
    return (head_body if sizes == [4, 4, 2] and whole and square else body)(*args)


def solution(mesh):
    return jax.shard_map(
        layer,
        mesh=mesh,
        in_specs=(
            P("fs", "sp", None),
            P("fs", "sp"),
            P("fs", "tp", None, None),
            P(),
            P(("sp", "fs"), "tp"),
            P(("sp", "fs"), "tp"),
            P(("sp", "fs"), "tp"),
            P(("sp", "fs"), "tp"),
            P(("sp", "fs"), "tp"),
            P(("sp", "fs"), "tp"),
            P(("sp", "fs"), "tp"),
            P(("sp", "fs"), "tp"),
            P(None, "tp"),
            P("tp"),
            P(),
            P("tp"),
            P("tp"),
            P("tp"),
            P("tp", ("sp", "fs")),
            P("tp", ("sp", "fs")),
        ),
        out_specs=P("fs", ("sp", "tp"), None),
        check_vma=False,
    )
```

```python
import functools

import jax
import jax.numpy as jnp
from jax import lax
from jax.experimental import pallas as pl
from jax.experimental.pallas import tpu as pltpu
from jax.sharding import PartitionSpec as P

NORM_FLOOR = 0.1
CHANNEL_FLOOR = 0.1
GROUP_FLOOR = 1.0
LANES = 128
SPAN = 64
SPARE = 16
BF = jnp.bfloat16
F32 = jnp.float32
VM = pl.BlockSpec(memory_space=pltpu.VMEM)


def dot_nn(a, b):
    return lax.dot_general(a, b, (((1,), (0,)), ((), ())), preferred_element_type=F32)


def dot_nt(a, b):
    return lax.dot_general(a, b, (((1,), (1,)), ((), ())), preferred_element_type=F32)


def dot_tn(a, b):
    return lax.dot_general(a, b, (((0,), (0,)), ((), ())), preferred_element_type=F32)


def sigmoid(x):
    return 1.0 / (1.0 + jnp.exp(-x))


def iota(shape, dim):
    return lax.broadcasted_iota(jnp.int32, shape, dim)


def three_terms(a):
    high = a.astype(BF).astype(F32)
    middle = (a - high).astype(BF).astype(F32)
    return high, middle, a - high - middle


def here():
    return [lax.axis_index(a) for a in ("sp", "fs", "tp")]


def split_weights_kernel(*refs):
    pace, convs, states, outs = refs[0], refs[1:4], refs[4:9], refs[9:]
    run = pace.shape[1] // 4
    paces = jnp.concatenate(
        [jnp.broadcast_to(pace[:, r * run : r * run + 1], (1, LANES // 2)) for r in range(4)], axis=0
    )
    rest = jnp.zeros((convs[0].shape[0] - 12, LANES // 2), F32)
    spare = jnp.concatenate([*three_terms(paces), rest], axis=0).astype(BF)
    half = LANES // 2
    z = here()[0]
    for step, out in enumerate(outs):
        target = z ^ step
        for at, ref in enumerate(states):
            out[:, at * LANES : (at + 1) * LANES] = ref[
                :, pl.ds(pl.multiple_of(target * LANES, LANES), LANES)
            ]
        odd = lax.rem(target, 2) == 1
        for at, ref in enumerate(convs):
            pair = ref[:, pl.ds(pl.multiple_of((target // 2) * LANES, LANES), LANES)]
            start = len(states) * LANES + at * half
            out[:, start : start + half] = jnp.where(odd, pair[:, half:], pair[:, :half])
        out[:, start + half :] = spare


def norm_kernel(tokens, gain, out_conv, out_state, conv_gain, normed, part, rows_out):
    count = part.shape[0]
    floats = tokens[...].astype(F32)
    inverse = lax.rsqrt(jnp.mean(floats * floats, axis=1, keepdims=True) + NORM_FLOOR)
    normed[...] = (floats * inverse * gain[...]).astype(BF)
    part[...] = normed[pl.ds(pl.multiple_of(here()[2] * count, 16), count), :]
    split, wide = out_conv.shape[0], out_state.shape[0]
    rows_out[:split, :] = out_conv[...]
    rows_out[split : split + wide, :] = out_state[...]
    gains = jnp.concatenate(
        [conv_gain[:, i * LANES : (i + 1) * LANES] for i in range(split // LANES)], axis=0
    )
    spare = jnp.concatenate(
        list(three_terms(gains)) + [jnp.zeros((SPARE - 3 * gains.shape[0], LANES), F32)],
        axis=0,
    )
    rows_out[split + wide :, :] = spare.astype(BF)


def assemble_kernel(*refs):
    *sources, out = refs
    size = sources[0].shape[0]
    for i, source in enumerate(sources):
        out[i * size : (i + 1) * size, :] = source[...]


def call(kernel, outs, *args, scratch=(), held=(), whole=(), room=10, **settings):
    specs, operands = [], []
    for at, arg in enumerate(args):
        specs.append(pl.BlockSpec(memory_space=pl.ANY) if at in whole else VM)
        apart = at in held or at in whole
        operands.append(pltpu.with_memory_space_constraint(arg, pltpu.HBM if apart else pltpu.VMEM))
    return pl.pallas_call(
        functools.partial(kernel, **settings) if settings else kernel,
        out_shape=[pltpu.VMEM(*o) if isinstance(o, tuple) else o for o in outs],
        in_specs=specs,
        out_specs=[VM] * len(outs),
        scratch_shapes=[pltpu.VMEM(*a) if isinstance(a, tuple) else a for a in scratch],
        compiler_params=pltpu.CompilerParams(vmem_limit_bytes=room << 20),
    )(*operands)


def masks():
    half = LANES // 2
    lane = iota((1, LANES), 1)
    first = (lane < half).astype(F32)
    ri, ci = iota((LANES, LANES), 0), iota((LANES, LANES), 1)
    return first, 1.0 - first, ri, ci, (ri // half) == (ci // half)


def stage_terms(x, w, paces, base_row, corr_row, conv_part, gate_part, local, lead, step, added, kept, proj, log_keep):
    length = x.shape[0]
    first, second, ri, ci, same = masks()
    sum_mat = jnp.where(same, 1.0, 0.0).astype(BF)
    strict = same & (ri > ci)
    weak = same & (ri >= ci)
    eye = jnp.where(ri == ci, 1.0, 0.0).astype(F32)
    run = length // 4
    proj[...] = dot_nn(x[...], w[...])
    gate_part[...] = proj[:, 4 * LANES : 5 * LANES].astype(BF)
    conv_part[...] = proj[:, 5 * LANES : 7 * LANES].astype(BF)
    rate = -jnp.exp(base_row + jnp.tanh(proj[:, 3 * LANES : 4 * LANES].astype(BF).astype(F32)))
    for r in range(4):
        log_keep[r * run : (r + 1) * run, :] = rate[r * run : (r + 1) * run, :] * paces[r : r + 1, :]

    chunks = length // SPAN
    tri = jnp.where(iota((SPAN, SPAN), 0) >= iota((SPAN, SPAN), 1), 1.0, 0.0).astype(F32)

    def stack(a):
        return jnp.concatenate([a * first, a * second], axis=0).astype(BF)

    sums = lax.dot_general(
        tri,
        jnp.concatenate([log_keep[c * SPAN : (c + 1) * SPAN, :] for c in range(chunks)], axis=1),
        (((1,), (0,)), ((), ())),
        precision=lax.Precision.HIGHEST,
        preferred_element_type=F32,
    )
    levels = []
    size = 1
    while size < SPAN:
        inside = (ri // (2 * size)) == (ci // (2 * size))
        levels.append(inside & ((ri & size) != 0) & ((ci & size) == 0))
        size *= 2
    grams, tails, heads = [], [], []
    for c in range(chunks):
        rows = slice(c * SPAN, (c + 1) * SPAN)
        total = sums[:, c * LANES : (c + 1) * LANES]
        before = total - log_keep[rows, :]
        last = total[SPAN - 1 : SPAN, :]
        q = proj[rows, 0:LANES].astype(BF).astype(F32)
        k = proj[rows, LANES : 2 * LANES].astype(BF).astype(F32)
        v = proj[rows, 2 * LANES : 3 * LANES]
        norm = dot_nn((k * k).astype(BF), sum_mat)
        unit = k * lax.rsqrt(jnp.maximum(norm, 1.0))
        write = unit * corr_row
        back = jnp.exp(-total)
        rest = jnp.exp(last - total)
        lead_remove = stack(-unit * jnp.exp(before))
        lead_query = stack(q * jnp.exp(total))
        grams.append(
            dot_nt(
                jnp.concatenate([lead_remove, lead_query], axis=0),
                jnp.concatenate([stack(write * back), stack(k * back)], axis=0),
            )
        )
        tails.append((stack(write * rest), stack(k * rest)))
        heads.append((lead_remove, lead_query, stack(v)))
        kept[c] = jnp.broadcast_to(jnp.exp(last), kept.shape[1:])
    system = [jnp.where(strict, g[:LANES, :LANES], 0.0) for g in grams]
    inverse = [eye + jnp.where(levels[0], a, 0.0) for a in system]
    for level in levels[1:]:
        low = [i.astype(BF) for i in inverse]
        inner = [
            dot_nn(i, jnp.where(level, a, 0.0).astype(BF)).astype(BF) for i, a in zip(low, system)
        ]
        inverse = [i + dot_nn(n, b) for i, n, b in zip(inverse, inner, low)]
    direct = [
        dot_nn(
            jnp.concatenate(
                [
                    jnp.where(strict, g[:LANES, LANES:], 0.0),
                    jnp.where(weak, g[LANES:, LANES:], 0.0),
                ],
                axis=0,
            ).astype(BF),
            h[2],
        )
        for g, h in zip(grams, heads)
    ]
    solved = [
        dot_nn(i.astype(BF), jnp.concatenate([d[:LANES].astype(BF), h[0]], axis=1)).astype(BF)
        for i, d, h in zip(inverse, direct, heads)
    ]
    through = [
        dot_nn(jnp.where(weak, g[LANES:, :LANES], 0.0).astype(BF), s) for g, s in zip(grams, solved)
    ]
    for c, (d, s, h, u, tail) in enumerate(zip(direct, solved, heads, through, tails)):
        own = u[:, :LANES] + d[LANES:]
        moved = dot_tn(s, tail[0])
        local[c] = own[:SPAN] + own[SPAN:]
        lead[c] = (h[1].astype(F32) + u[:, LANES:]).astype(BF)
        step[c] = moved[LANES:].astype(BF)
        added[c] = moved[:LANES] + dot_tn(h[2], tail[1])


def own_kernel(x, mine, sibling, base, correction, w, *outs):
    z, f, _ = here()
    count = lax.axis_size("sp")
    for i in range(mine.shape[0] // LANES):
        level, step = i // count, i % count
        source = z ^ step
        for ref, flip in ((mine, 0), (sibling, 1)):
            row = (source * lax.axis_size("fs") + (f ^ (2 * level) ^ flip)) * LANES
            w[pl.ds(pl.multiple_of(row, LANES), LANES), :] = ref[i * LANES : (i + 1) * LANES, :]
    block_terms_in(z, x, w, base, correction, outs)


def block_terms_in(position, x, w, base, correction, refs):
    row = (position * lax.axis_size("fs") + here()[1]) * LANES
    spare = w[pl.ds(pl.multiple_of(row, LANES), 16), w.shape[1] - LANES :].astype(F32)
    paces = spare[0:4, :] + spare[4:8, :] + spare[8:12, :]
    paces = jnp.concatenate([paces[:, LANES // 2 :]] * 2, axis=1)
    stage_terms(x, w, paces, base[...], correction[...], *refs)


def prepare_kernel(start, base, correction, group_gain, taps, state, *outs):
    z = here()[0]
    half = LANES // 2
    column = pl.ds(pl.multiple_of(z * LANES, LANES), LANES)
    *rows, tap_rows = outs
    for row, ref in zip(rows, (base, correction, group_gain)):
        row[...] = ref[:, column]
    zero = jnp.zeros((half, half), F32)
    state[:half, :] = jnp.concatenate([start[2 * z], zero], axis=1)
    state[half:, :] = jnp.concatenate([zero, start[2 * z + 1]], axis=1)
    tap = taps[:, pl.ds(pl.multiple_of((z // 2) * LANES, LANES), LANES)]
    tap_rows[: taps.shape[0], :] = tap


def block_kernel(*refs, step, conditions):
    count = len(conditions)
    sources = refs[: 2 * count]
    w, base, correction = refs[2 * count : 2 * count + 3]
    *outs, proj, log_keep, x = refs[2 * count + 3 :]
    z, _, t = here()
    part = x.shape[0] // 2
    for at, holds in enumerate(conditions):
        a, b = sources[2 * at : 2 * at + 2]

        def put(a=a, b=b):
            x[pl.ds(pl.multiple_of(t * part, 32), part), :] = a[...]
            x[pl.ds(pl.multiple_of((1 - t) * part, 32), part), :] = b[...]

        put() if holds is None else pl.when(holds(z))(put)
    block_terms_in(z ^ step, x, w, base, correction, (*outs, proj, log_keep))


def final_kernel(*refs, count, width):
    slots = [refs[7 * i : 7 * (i + 1)] for i in range(count)]
    start, rows_in, tap, out, conv, gates, local, lead, step, added, kept, conv_rows, y = refs[
        7 * count :
    ]
    z = here()[0]
    half = LANES // 2
    first, second, _, _, same = masks()
    mean_mat = jnp.where(same, 1.0 / half, 0.0).astype(BF)
    length = conv.shape[1]
    total_rows = count * length
    for at, slot in enumerate(slots):
        position = z ^ at
        for target, source in zip((conv, gates, local, lead, step, added, kept), slot):
            target[position] = source[...]

    middle = total_rows // 2
    pad = conv_rows.shape[0] - middle
    for block in range(count):
        pair = conv[block, :, :LANES].astype(F32)
        conv_in = (pair * pltpu.roll(sigmoid(pair), half, 1)).astype(BF).astype(F32)
        at = block * length
        if at < middle:
            conv_rows[pad + at : pad + at + length, :] = conv_in * first
            if at + length == middle:
                conv_rows[:pad, :] = pltpu.roll(conv_in[length - pad :, :], half, 1) * second
        else:
            rows = slice(pad + at - middle, pad + at - middle + length)
            conv_rows[rows, :] = conv_rows[rows, :] + pltpu.roll(conv_in, half, 1) * second
        out[at : at + length, LANES + half : 2 * LANES] = conv[block, :, LANES : LANES + half]
    tap = tap[:width, :]
    odd = (lax.rem(z, 2) == 1).astype(F32)
    left = iota((1, LANES), 1) < half
    tap = jnp.where(left == (odd < 0.5), tap, pltpu.roll(tap, half, 1))
    shift = pad - (width - 1)
    strip = 96
    for at in range(0, middle, strip):
        total = jnp.zeros((strip, LANES), F32)
        for j in range(width):
            total = total + tap[j : j + 1, :] * conv_rows[at + shift + j : at + shift + j + strip, :]
        total = total.astype(BF)
        out[at : at + strip, LANES : LANES + half] = total[:, :half]
        out[middle + at : middle + at + strip, LANES : LANES + half] = total[:, half:]

    state = start[...]
    chunks = length // SPAN
    for c in range(count * chunks):
        at = (c // chunks, c % chunks)
        low = state.astype(BF)
        seen = dot_nt(lead[at], low)
        y[c * SPAN : (c + 1) * SPAN, :] = local[at] + seen[:SPAN] + seen[SPAN:]
        state = state * kept[at][:1] + dot_nn(low, step[at]) + added[at]

    gain_row = rows_in[...]
    for block in range(count):
        rows = slice(block * length, (block + 1) * length)
        values = y[rows, :]
        high = values.astype(BF)
        low = (values - high.astype(F32)).astype(BF)
        centered = values - (dot_nn(high, mean_mat) + dot_nn(low, mean_mat))
        variance = dot_nn((centered * centered).astype(BF), mean_mat)
        gate = gates[block].astype(F32)
        grouped = centered * lax.rsqrt(variance + GROUP_FLOOR) * gain_row
        out[rows, :LANES] = (grouped * (gate * sigmoid(gate))).astype(BF)


def join_kernel(*refs, groups):
    *pieces, w, all_gains = refs
    _, f, t = here()
    count = pieces[0].shape[0]
    split = count * LANES // 2
    wide = count * LANES
    gains = []
    for at, piece in enumerate(pieces):
        core, flip, side = at & 1, (at >> 1) & 1, (at >> 2) & 1
        group = t ^ side
        for block in range(count):
            col = pl.multiple_of((block * count + (f ^ (2 * flip) ^ core)) * LANES, LANES)
            for start, size, shift in (
                (0, split, group * split),
                (split, wide, groups * split + group * wide),
            ):
                w[pl.ds(pl.multiple_of(shift, LANES), size), pl.ds(col, LANES)] = piece[
                    block, start : start + size, :
                ]
        if core == flip == 0:
            spare = piece[0, split + wide :, :].astype(F32)
            tall = split // LANES
            parts = [spare[i * tall : (i + 1) * tall, :] for i in range(3)]
            total = parts[0] + parts[1] + parts[2]
            gains.append(jnp.concatenate([total[i : i + 1] for i in range(tall)], axis=1))
    all_gains[...] = jnp.concatenate(
        [jnp.where(t == 0, gains[0], gains[1]), jnp.where(t == 0, gains[1], gains[0])], axis=1
    )


def output_kernel(received, point, gain, rows_in, out, w, sems, *, groups):
    count = received.shape[0] // groups
    wide = w.shape[1] // count
    columns = [pl.ds(i * wide, wide) for i in range(count)]
    copies = [
        pltpu.make_async_copy(rows_in.at[:, c], w.at[:, c], sems.at[i]) for i, c in enumerate(columns)
    ]
    for copy in copies:
        copy.start()
    half = LANES // 2
    sums, gates, states = [], [], []
    for group in range(groups):
        for block in range(count):
            source = received[block * groups + group]
            states.append(source[:, :LANES])
            sums.append(source[:, LANES : LANES + half])
            gates.append(source[:, LANES + half :])
    conv_sum = jnp.concatenate(sums, axis=1).astype(F32)
    gate = jnp.concatenate(gates, axis=1).astype(F32)
    mean = jnp.mean(conv_sum, axis=1, keepdims=True)
    spread = jnp.mean(conv_sum * conv_sum, axis=1, keepdims=True) - mean * mean
    scaled = (conv_sum - mean) * lax.rsqrt(spread + CHANNEL_FLOOR) * gain[...]
    shaped = (scaled * sigmoid(scaled)).astype(BF)
    conv_out = (dot_nn(shaped, point[...]) * (gate * sigmoid(gate))).astype(BF)
    joined = jnp.concatenate([conv_out] + states, axis=1)
    for c, copy in zip(columns, copies):
        copy.wait()
        out[:, c] = dot_nn(joined, w[:, c]).astype(BF)


def ordered_kernel(own, *refs):
    *sources, out = refs
    z = here()[0]
    out[z] = own[...]
    for step, choices in ARRIVALS:
        for at, holds in choices:

            def put(step=step, at=at):
                out[z ^ step] = sources[at][...]

            put() if holds is None else pl.when(holds(z))(put)


LINE = (
    ((0, 1), (1, 0), (2, 3), (3, 2)),
    ((0, 2), (1, 3), (2, 0), (3, 1)),
    ((1, 2), (2, 1)),
    ((2, 3), (1, 0)),
)
FORWARD = {3: 1}


def inner(z):
    return (z == 1) | (z == 2)


def outer(z):
    return (z == 0) | (z == 3)


ARRIVALS = (
    (1, ((0, None),)),
    (2, ((1, None),)),
    (3, ((2, inner), (3, outer))),
)


def along_line(value):
    moved = []
    for i, pairs in enumerate(LINE):
        moved.append(lax.ppermute(moved[FORWARD[i]] if i in FORWARD else value, "sp", pairs))
    return moved


def across(value, pairs):
    targets = sorted({b for _, b in pairs})
    return lax.ppermute(
        value, ("sp", "tp"), [(2 * i + s, 2 * i + 1 - s) for i in targets for s in (0, 1)]
    )


def flipped(value, axis, bit):
    count = lax.axis_size(axis)
    return lax.ppermute(value, axis, [(i, i ^ bit) for i in range(count)])


def head_body(
    tokens, decay_pace, start_state, norm_gain, conv_value, conv_admit, conv_gate, state_query,
    state_key, state_value, state_decay, state_gate, conv_taps, conv_gain, point_weight, decay_base,
    correction, group_gain, output_conv, output_state,
):
    width = tokens.shape[-1]
    length = tokens.shape[1]
    count, halves = lax.axis_size("sp"), lax.axis_size("tp")
    part = length // halves
    shard = conv_value.shape[0]
    columns = 7 * LANES
    slices = call(
        split_weights_kernel, [((shard, columns), BF)] * count,
        decay_pace, conv_value, conv_admit, conv_gate, state_query, state_key, state_value, state_decay,
        state_gate, held=range(9),
    )
    taken = [slices[0]] + [flipped(slices[k], "sp", k) for k in range(1, count)]
    out_rows = output_conv.shape[0] + output_state.shape[0]
    normed, half, rows_out = call(
        norm_kernel,
        [pltpu.HBM((length, width), BF), ((part, width), BF), ((out_rows + SPARE, output_conv.shape[1]), BF)],
        tokens.reshape(length, width), norm_gain.reshape(1, width), output_conv,
        output_state, conv_gain.reshape(1, -1), held=range(5),
    )
    line_out = along_line(rows_out)
    near = along_line(half)
    far = [across(a, LINE[i]) for i, a in enumerate(near)]
    lifted = [flipped(a, "fs", 2) for a in taken]
    (mine,) = call(assemble_kernel, [((2 * count * shard, columns), BF)], *taken, *lifted)
    sibling = flipped(mine, "fs", 1)
    (ordered,) = call(ordered_kernel, [((count,) + rows_out.shape, BF)], rows_out, *line_out)
    crossed = flipped(ordered, "tp", 1)
    pieces = []
    for a in (ordered, crossed):
        for b in (a, flipped(a, "fs", 2)):
            pieces += [b, flipped(b, "fs", 1)]
    total = length * count
    rows = total // (count * halves)
    chunks = length // SPAN
    terms = [
        ((length, 2 * LANES), BF),
        ((length, LANES), BF),
        ((chunks, SPAN, LANES), F32),
        ((chunks, LANES, LANES), BF),
        ((chunks, LANES, LANES), BF),
        ((chunks, LANES, LANES), F32),
        ((chunks, 8, LANES), F32),
    ]
    work = [((length, columns), F32), ((length, LANES), F32)]
    heads = start_state.shape[1]
    kernel = conv_taps.shape[0]
    begin, *small, gains, tap = call(
        prepare_kernel,
        [((LANES, LANES), F32)] + [((1, LANES), F32)] * 3 + [((-(-kernel // 8) * 8, LANES), F32)],
        start_state.reshape(heads, *start_state.shape[2:]), decay_base.reshape(1, -1),
        correction.reshape(1, -1), group_gain.reshape(1, -1), conv_taps, held=range(5),
    )
    w, *slots = call(
        own_kernel, [((width, columns), BF)] + terms,
        normed, mine, sibling, *small, held=(0,), scratch=work,
    )
    for step, choices in ARRIVALS:
        sources = [a for i, _ in choices for a in (near[i], far[i])]
        slots += call(
            block_kernel, terms, *sources, w, *small,
            scratch=work + [((length, width), BF)],
            step=step, conditions=tuple(holds for _, holds in choices),
        )
    mixed = call(
        final_kernel, [((total, 2 * LANES), BF)], *slots, begin, gains, tap,
        count=count, width=kernel,
        scratch=[((count,) + a, b) for a, b in terms]
        + [((total // 2 + 32, LANES), F32), ((total, LANES), F32)],
    )[0]
    received = lax.all_to_all(
        mixed.reshape(count * halves, rows, 2 * LANES), ("sp", "tp"), 0, 0, tiled=True
    )
    w_out, gain = call(
        join_kernel,
        [
            pltpu.HBM((halves * out_rows, width), BF),
            ((1, halves * conv_gain.shape[0]), F32),
        ],
        *pieces, room=20, groups=halves,
    )
    (out,) = call(
        output_kernel, [jax.ShapeDtypeStruct((rows, width), BF)],
        received, point_weight, gain, w_out, whole=(3,), room=12, groups=halves,
        scratch=[((halves * out_rows, width), BF), pltpu.SemaphoreType.DMA((count,))],
    )
    return out.reshape(1, rows, width)


def passed_along(value, axis, steps):
    count = lax.axis_size(axis)
    leading, last = (max(0, -steps), min(count, count - steps))
    return lax.ppermute(value, axis, [(source, source + steps) for source in range(leading, last)])


def entering_2(value, axis, join, neutral):
    place = lax.axis_index(axis)
    gathered = jax.tree.map(
        lambda a, kind: lax.all_gather(a.astype(kind), axis),
        value,
        jax.tree.map(lambda a: jnp.bfloat16 if a.dtype == jnp.float32 else a.dtype, value),
    )
    state = jax.tree.map(lambda a, e: jnp.zeros_like(a) + jnp.asarray(e, a.dtype), value, neutral)

    def one(lap, state):
        return join(
            state,
            jax.tree.map(
                lambda a, own: lax.dynamic_index_in_dim(a, lap, 0, False).astype(own.dtype),
                gathered,
                value,
            ),
        )

    return lax.fori_loop(0, place, one, state)


def apply_map(matrix, right):
    return jnp.einsum("hbti,hbic->hbtc", matrix, right, precision=lax.Precision.HIGHEST)


def pair_terms(left, right, mask):
    return jnp.einsum("hbtc,hbic->hbti", left, right, precision=lax.Precision.HIGHEST) * mask


def compose(earlier, later):
    first = jnp.matmul(earlier[0], later[0], precision=lax.Precision.HIGHEST)
    second = jnp.matmul(earlier[1], later[0], precision=lax.Precision.HIGHEST) + later[1]
    return (first, second)


def block_terms(query, keys, values, unit, write, log_keep):
    size = query.shape[-1]
    span = query.shape[2]
    total_log = jnp.cumsum(log_keep, axis=2)
    before_log = total_log - log_keep
    last_log = total_log[:, :, span - 1 :, :]
    lead_remove = -unit * jnp.exp(before_log)
    lead_query = query * jnp.exp(total_log)
    back_write = write * jnp.exp(-total_log)
    back_key = keys * jnp.exp(-total_log)
    places = jnp.arange(span)
    strict = (places[:, None] > places[None, :]).astype(jnp.float32)
    weak = (places[:, None] >= places[None, :]).astype(jnp.float32)
    remove_write = pair_terms(lead_remove, back_write, strict)
    remove_key = pair_terms(lead_remove, back_key, strict)
    query_write = pair_terms(lead_query, back_write, weak)
    query_key = pair_terms(lead_query, back_key, weak)
    right_side = jnp.concatenate([apply_map(remove_key, values), lead_remove], axis=-1)
    system = jnp.eye(span, dtype=jnp.float32) - remove_write
    solved = jax.scipy.linalg.solve_triangular(system, right_side, lower=True, unit_diagonal=True)
    own_part = solved[..., :size]
    start_part = solved[..., size:]
    local_out = apply_map(query_write, own_part) + apply_map(query_key, values)
    start_map = lead_query + apply_map(query_write, start_part)
    tail_write = write * jnp.exp(last_log - total_log)
    tail_key = keys * jnp.exp(last_log - total_log)
    carry_map = jnp.einsum(
        "hbtk,hbtj->hbkj", start_part, tail_write, precision=lax.Precision.HIGHEST
    ) + jnp.eye(size, dtype=jnp.float32) * jnp.exp(last_log)
    carry_add = jnp.einsum(
        "hbtv,hbtj->hbvj", own_part, tail_write, precision=lax.Precision.HIGHEST
    ) + jnp.einsum("hbtv,hbtj->hbvj", values, tail_key, precision=lax.Precision.HIGHEST)
    return (local_out, start_map, carry_map, carry_add)


def body(
    tokens,
    decay_pace,
    start_state,
    norm_gain,
    conv_value,
    conv_admit,
    conv_gate,
    state_query,
    state_key,
    state_value,
    state_decay,
    state_gate,
    conv_taps,
    conv_gain,
    point_weight,
    decay_base,
    correction,
    group_gain,
    output_conv,
    output_state,
):
    width = tokens.shape[-1]
    rows = tokens.reshape(-1, width)
    length = rows.shape[0]
    floats = rows.astype(jnp.float32)
    inverse = lax.rsqrt(jnp.mean(floats * floats, axis=1, keepdims=True) + NORM_FLOOR)
    normed = (floats * inverse * norm_gain).astype(jnp.bfloat16)
    shards = (
        conv_value,
        conv_admit,
        conv_gate,
        state_query,
        state_key,
        state_value,
        state_decay,
        state_gate,
    )
    stacked = jnp.concatenate(shards, axis=1)
    projected = jnp.dot(
        normed,
        lax.all_gather(stacked, ("sp", "fs"), axis=0, tiled=True),
        preferred_element_type=jnp.float32,
    ).astype(jnp.bfloat16)
    pieces = []
    offset = 0
    for shard in shards:
        pieces.append(projected[:, offset : offset + shard.shape[1]].astype(jnp.float32))
        offset = offset + shard.shape[1]
    value, admit, gate_conv, query, keys, values, decay_in, gate_state = pieces
    channels = value.shape[1]
    kernel = conv_taps.shape[0]
    conv_input = (value * jax.nn.sigmoid(admit)).astype(jnp.bfloat16)
    earlier = passed_along(conv_input[length - (kernel - 1) :], "sp", 1)
    padded = jnp.concatenate([earlier, conv_input], axis=0).astype(jnp.float32)
    conv_sum = jnp.zeros((length, channels), jnp.float32)
    for place in range(kernel):
        conv_sum = conv_sum + conv_taps[place] * padded[place : place + length]
    local_point = lax.dynamic_slice_in_dim(
        point_weight, lax.axis_index("tp") * channels, channels, 1
    )
    whole_sum, whole_gain = (
        lax.all_gather(conv_sum.astype(jnp.bfloat16), "tp", axis=1, tiled=True).astype(
            conv_sum.dtype
        ),
        lax.all_gather(conv_gain.astype(jnp.bfloat16), "tp", axis=0, tiled=True).astype(
            conv_gain.dtype
        ),
    )
    mean = jnp.mean(whole_sum, axis=1, keepdims=True)
    spread = jnp.mean(whole_sum * whole_sum, axis=1, keepdims=True) - mean * mean
    shaped = jax.nn.silu(
        (whole_sum - mean) * lax.rsqrt(spread + CHANNEL_FLOOR) * whole_gain
    ).astype(jnp.bfloat16)
    pointwise = jnp.dot(shaped, local_point, preferred_element_type=jnp.float32)
    conv_out = (pointwise * jax.nn.silu(gate_conv)).astype(jnp.bfloat16)
    size = start_state.shape[-1]
    heads = query.shape[1] // size
    span = min(64, length)
    blocks = length // span
    log_keep = -jnp.exp(decay_base + jnp.tanh(decay_in)) * decay_pace.reshape(-1)[:, None]
    key_heads = keys.reshape(length, heads, size)
    unit = key_heads * lax.rsqrt(
        jnp.maximum(jnp.sum(key_heads * key_heads, axis=-1, keepdims=True), 1.0)
    )
    write = unit * correction.reshape(heads, size)

    def arrange(array):
        return array.reshape(blocks, span, heads, size).transpose(2, 0, 1, 3)

    local_out, start_map, carry_map, carry_add = block_terms(
        arrange(query),
        arrange(keys),
        arrange(values),
        arrange(unit),
        arrange(write),
        arrange(log_keep),
    )
    identity = (
        jnp.broadcast_to(jnp.eye(size, dtype=jnp.float32), (heads, size, size)),
        jnp.zeros((heads, size, size), jnp.float32),
    )

    def along(carried, block_pair):
        return (compose(carried, block_pair), carried)

    device_pair, prefixes = lax.scan(
        along, identity, (jnp.moveaxis(carry_map, 1, 0), jnp.moveaxis(carry_add, 1, 0))
    )
    prior_map, prior_add = entering_2(device_pair, "sp", compose, identity)
    begin = start_state.reshape(heads, size, size)
    entering = jnp.matmul(begin, prior_map, precision=lax.Precision.HIGHEST) + prior_add
    block_starts = (
        jnp.matmul(entering[None], prefixes[0], precision=lax.Precision.HIGHEST) + prefixes[1]
    )
    block_starts = jnp.moveaxis(block_starts, 0, 1)
    outputs = local_out + jnp.einsum(
        "hbtk,hbvk->hbtv", start_map, block_starts, precision=lax.Precision.HIGHEST
    )
    outputs = outputs.transpose(1, 2, 0, 3).reshape(length, heads, size)
    centered = outputs - jnp.mean(outputs, axis=-1, keepdims=True)
    variance = jnp.mean(centered * centered, axis=-1, keepdims=True)
    grouped = centered * lax.rsqrt(variance + GROUP_FLOOR) * group_gain.reshape(heads, size)
    state_out = (grouped.reshape(length, heads * size) * jax.nn.silu(gate_state)).astype(
        jnp.bfloat16
    )
    local_mix = jnp.concatenate([conv_out, state_out], axis=1)
    moved = lax.all_to_all(local_mix, "tp", split_axis=0, concat_axis=1, tiled=True)
    conv_rows, state_rows = (
        lax.all_gather(output_conv, "tp", axis=0, tiled=True),
        lax.all_gather(output_state, "tp", axis=0, tiled=True),
    )
    groups = lax.axis_size("tp")
    joined = jnp.concatenate(
        [conv_rows.reshape(groups, channels, -1), state_rows.reshape(groups, heads * size, -1)],
        axis=1,
    )
    joined = joined.reshape(groups * (channels + heads * size), -1)
    mixed = jnp.dot(
        moved,
        lax.all_gather(joined, ("sp", "fs"), axis=1, tiled=True),
        preferred_element_type=jnp.float32,
    )
    return mixed.astype(jnp.bfloat16).reshape(1, -1, width)


def layer(*args):
    sizes = [lax.axis_size(a) for a in ("sp", "fs", "tp")]
    channels, wide = args[4].shape[1], args[7].shape[1]
    whole = channels == sizes[0] * LANES // 2 and wide == sizes[0] * LANES
    square = args[2].shape[-1] == LANES // 2 and args[4].shape[0] == LANES
    return (head_body if sizes == [4, 4, 2] and whole and square else body)(*args)


def solution(mesh):
    return jax.shard_map(
        layer,
        mesh=mesh,
        in_specs=(
            P("fs", "sp", None),
            P("fs", "sp"),
            P("fs", "tp", None, None),
            P(),
            P(("sp", "fs"), "tp"),
            P(("sp", "fs"), "tp"),
            P(("sp", "fs"), "tp"),
            P(("sp", "fs"), "tp"),
            P(("sp", "fs"), "tp"),
            P(("sp", "fs"), "tp"),
            P(("sp", "fs"), "tp"),
            P(("sp", "fs"), "tp"),
            P(None, "tp"),
            P("tp"),
            P(),
            P("tp"),
            P("tp"),
            P("tp"),
            P("tp", ("sp", "fs")),
            P("tp", ("sp", "fs")),
        ),
        out_specs=P("fs", ("sp", "tp"), None),
        check_vma=False,
    )
```

```python
import functools

import jax
import jax.numpy as jnp
from jax import lax
from jax.experimental import pallas as pl
from jax.experimental.pallas import tpu as pltpu
from jax.sharding import PartitionSpec as P

NORM_FLOOR = 0.1
CHANNEL_FLOOR = 0.1
GROUP_FLOOR = 1.0
LANES = 128
SPAN = 64
SPARE = 16
BF = jnp.bfloat16
F32 = jnp.float32
VM = pl.BlockSpec(memory_space=pltpu.VMEM)


def dot_nn(a, b):
    return lax.dot_general(a, b, (((1,), (0,)), ((), ())), preferred_element_type=F32)


def dot_nt(a, b):
    return lax.dot_general(a, b, (((1,), (1,)), ((), ())), preferred_element_type=F32)


def dot_tn(a, b):
    return lax.dot_general(a, b, (((0,), (0,)), ((), ())), preferred_element_type=F32)


def sigmoid(x):
    return 1.0 / (1.0 + jnp.exp(-x))


def iota(shape, dim):
    return lax.broadcasted_iota(jnp.int32, shape, dim)


def three_terms(a):
    high = a.astype(BF).astype(F32)
    middle = (a - high).astype(BF).astype(F32)
    return high, middle, a - high - middle


def here():
    return [lax.axis_index(a) for a in ("sp", "fs", "tp")]


def split_weights_kernel(*refs):
    pace, convs, states, outs = refs[0], refs[1:4], refs[4:9], refs[9:]
    run = pace.shape[1] // 4
    paces = jnp.concatenate(
        [jnp.broadcast_to(pace[:, r * run : r * run + 1], (1, LANES // 2)) for r in range(4)], axis=0
    )
    rest = jnp.zeros((convs[0].shape[0] - 12, LANES // 2), F32)
    spare = jnp.concatenate([*three_terms(paces), rest], axis=0).astype(BF)
    half = LANES // 2
    z = here()[0]
    for step, out in enumerate(outs):
        target = z ^ step
        for at, ref in enumerate(states):
            out[:, at * LANES : (at + 1) * LANES] = ref[
                :, pl.ds(pl.multiple_of(target * LANES, LANES), LANES)
            ]
        odd = lax.rem(target, 2) == 1
        for at, ref in enumerate(convs):
            pair = ref[:, pl.ds(pl.multiple_of((target // 2) * LANES, LANES), LANES)]
            start = len(states) * LANES + at * half
            out[:, start : start + half] = jnp.where(odd, pair[:, half:], pair[:, :half])
        out[:, start + half :] = spare


def rows_kernel(out_conv, out_state, conv_gain, rows_out):
    split, wide = out_conv.shape[0], out_state.shape[0]
    rows_out[:split, :] = out_conv[...]
    rows_out[split : split + wide, :] = out_state[...]
    gains = jnp.concatenate(
        [conv_gain[:, i * LANES : (i + 1) * LANES] for i in range(split // LANES)], axis=0
    )
    spare = jnp.concatenate(
        list(three_terms(gains)) + [jnp.zeros((SPARE - 3 * gains.shape[0], LANES), F32)],
        axis=0,
    )
    rows_out[split + wide :, :] = spare.astype(BF)


def norm_kernel(tokens, gain, normed, part):
    count = part.shape[0]
    floats = tokens[...].astype(F32)
    inverse = lax.rsqrt(jnp.mean(floats * floats, axis=1, keepdims=True) + NORM_FLOOR)
    normed[...] = (floats * inverse * gain[...]).astype(BF)
    part[...] = normed[pl.ds(pl.multiple_of(here()[2] * count, 16), count), :]


def assemble_kernel(*refs):
    *sources, out = refs
    size = sources[0].shape[0]
    for i, source in enumerate(sources):
        out[i * size : (i + 1) * size, :] = source[...]


def call(kernel, outs, *args, scratch=(), held=(), whole=(), room=10, **settings):
    specs, operands = [], []
    for at, arg in enumerate(args):
        specs.append(pl.BlockSpec(memory_space=pl.ANY) if at in whole else VM)
        apart = at in held or at in whole
        operands.append(pltpu.with_memory_space_constraint(arg, pltpu.HBM if apart else pltpu.VMEM))
    return pl.pallas_call(
        functools.partial(kernel, **settings) if settings else kernel,
        out_shape=[pltpu.VMEM(*o) if isinstance(o, tuple) else o for o in outs],
        in_specs=specs,
        out_specs=[VM] * len(outs),
        scratch_shapes=[pltpu.VMEM(*a) if isinstance(a, tuple) else a for a in scratch],
        compiler_params=pltpu.CompilerParams(vmem_limit_bytes=room << 20),
    )(*operands)


def masks():
    half = LANES // 2
    lane = iota((1, LANES), 1)
    first = (lane < half).astype(F32)
    ri, ci = iota((LANES, LANES), 0), iota((LANES, LANES), 1)
    return first, 1.0 - first, ri, ci, (ri // half) == (ci // half)


def stage_terms(x, w, paces, base_row, corr_row, conv_part, gate_part, local, lead, step, added, kept, proj, log_keep):
    length = x.shape[0]
    first, second, ri, ci, same = masks()
    sum_mat = jnp.where(same, 1.0, 0.0).astype(BF)
    strict = same & (ri > ci)
    weak = same & (ri >= ci)
    eye = jnp.where(ri == ci, 1.0, 0.0).astype(F32)
    run = length // 4
    proj[...] = dot_nn(x[...], w[...])
    gate_part[...] = proj[:, 4 * LANES : 5 * LANES].astype(BF)
    conv_part[...] = proj[:, 5 * LANES : 7 * LANES].astype(BF)
    rate = -jnp.exp(base_row + jnp.tanh(proj[:, 3 * LANES : 4 * LANES].astype(BF).astype(F32)))
    for r in range(4):
        log_keep[r * run : (r + 1) * run, :] = rate[r * run : (r + 1) * run, :] * paces[r : r + 1, :]

    chunks = length // SPAN
    tri = jnp.where(iota((SPAN, SPAN), 0) >= iota((SPAN, SPAN), 1), 1.0, 0.0).astype(F32)

    def stack(a):
        return jnp.concatenate([a * first, a * second], axis=0).astype(BF)

    sums = lax.dot_general(
        tri,
        jnp.concatenate([log_keep[c * SPAN : (c + 1) * SPAN, :] for c in range(chunks)], axis=1),
        (((1,), (0,)), ((), ())),
        precision=lax.Precision.HIGHEST,
        preferred_element_type=F32,
    )
    levels = []
    size = 1
    while size < SPAN:
        inside = (ri // (2 * size)) == (ci // (2 * size))
        levels.append(inside & ((ri & size) != 0) & ((ci & size) == 0))
        size *= 2
    grams, tails, heads = [], [], []
    for c in range(chunks):
        rows = slice(c * SPAN, (c + 1) * SPAN)
        total = sums[:, c * LANES : (c + 1) * LANES]
        before = total - log_keep[rows, :]
        last = total[SPAN - 1 : SPAN, :]
        q = proj[rows, 0:LANES].astype(BF).astype(F32)
        k = proj[rows, LANES : 2 * LANES].astype(BF).astype(F32)
        v = proj[rows, 2 * LANES : 3 * LANES]
        norm = dot_nn((k * k).astype(BF), sum_mat)
        unit = k * lax.rsqrt(jnp.maximum(norm, 1.0))
        write = unit * corr_row
        back = jnp.exp(-total)
        rest = jnp.exp(last - total)
        lead_remove = stack(-unit * jnp.exp(before))
        lead_query = stack(q * jnp.exp(total))
        grams.append(
            dot_nt(
                jnp.concatenate([lead_remove, lead_query], axis=0),
                jnp.concatenate([stack(write * back), stack(k * back)], axis=0),
            )
        )
        tails.append((stack(write * rest), stack(k * rest)))
        heads.append((lead_remove, lead_query, stack(v)))
        kept[c] = jnp.broadcast_to(jnp.exp(last), kept.shape[1:])
    system = [jnp.where(strict, g[:LANES, :LANES], 0.0) for g in grams]
    inverse = [eye + jnp.where(levels[0], a, 0.0) for a in system]
    for level in levels[1:]:
        low = [i.astype(BF) for i in inverse]
        inner = [
            dot_nn(i, jnp.where(level, a, 0.0).astype(BF)).astype(BF) for i, a in zip(low, system)
        ]
        inverse = [i + dot_nn(n, b) for i, n, b in zip(inverse, inner, low)]
    direct = [
        dot_nn(
            jnp.concatenate(
                [
                    jnp.where(strict, g[:LANES, LANES:], 0.0),
                    jnp.where(weak, g[LANES:, LANES:], 0.0),
                ],
                axis=0,
            ).astype(BF),
            h[2],
        )
        for g, h in zip(grams, heads)
    ]
    solved = [
        dot_nn(i.astype(BF), jnp.concatenate([d[:LANES].astype(BF), h[0]], axis=1)).astype(BF)
        for i, d, h in zip(inverse, direct, heads)
    ]
    through = [
        dot_nn(jnp.where(weak, g[LANES:, :LANES], 0.0).astype(BF), s) for g, s in zip(grams, solved)
    ]
    for c, (d, s, h, u, tail) in enumerate(zip(direct, solved, heads, through, tails)):
        own = u[:, :LANES] + d[LANES:]
        moved = dot_tn(s, tail[0])
        local[c] = own[:SPAN] + own[SPAN:]
        lead[c] = (h[1].astype(F32) + u[:, LANES:]).astype(BF)
        step[c] = moved[LANES:].astype(BF)
        added[c] = moved[:LANES] + dot_tn(h[2], tail[1])


def own_kernel(x, mine, sibling, base, correction, w, *outs):
    z, f, _ = here()
    count = lax.axis_size("sp")
    for i in range(mine.shape[0] // LANES):
        level, step = i // count, i % count
        source = z ^ step
        for ref, flip in ((mine, 0), (sibling, 1)):
            row = (source * lax.axis_size("fs") + (f ^ (2 * level) ^ flip)) * LANES
            w[pl.ds(pl.multiple_of(row, LANES), LANES), :] = ref[i * LANES : (i + 1) * LANES, :]
    block_terms_in(z, x, w, base, correction, outs)


def block_terms_in(position, x, w, base, correction, refs):
    row = (position * lax.axis_size("fs") + here()[1]) * LANES
    spare = w[pl.ds(pl.multiple_of(row, LANES), 16), w.shape[1] - LANES :].astype(F32)
    paces = spare[0:4, :] + spare[4:8, :] + spare[8:12, :]
    paces = jnp.concatenate([paces[:, LANES // 2 :]] * 2, axis=1)
    stage_terms(x, w, paces, base[...], correction[...], *refs)


def prepare_kernel(start, base, correction, group_gain, taps, state, *outs):
    z = here()[0]
    half = LANES // 2
    column = pl.ds(pl.multiple_of(z * LANES, LANES), LANES)
    *rows, tap_rows = outs
    for row, ref in zip(rows, (base, correction, group_gain)):
        row[...] = ref[:, column]
    zero = jnp.zeros((half, half), F32)
    state[:half, :] = jnp.concatenate([start[2 * z], zero], axis=1)
    state[half:, :] = jnp.concatenate([zero, start[2 * z + 1]], axis=1)
    tap = taps[:, pl.ds(pl.multiple_of((z // 2) * LANES, LANES), LANES)]
    tap_rows[: taps.shape[0], :] = tap


def block_kernel(*refs, step, conditions):
    count = len(conditions)
    sources = refs[: 2 * count]
    w, base, correction = refs[2 * count : 2 * count + 3]
    *outs, proj, log_keep, x = refs[2 * count + 3 :]
    z, _, t = here()
    part = x.shape[0] // 2
    for at, holds in enumerate(conditions):
        a, b = sources[2 * at : 2 * at + 2]

        def put(a=a, b=b):
            x[pl.ds(pl.multiple_of(t * part, 32), part), :] = a[...]
            x[pl.ds(pl.multiple_of((1 - t) * part, 32), part), :] = b[...]

        put() if holds is None else pl.when(holds(z))(put)
    block_terms_in(z ^ step, x, w, base, correction, (*outs, proj, log_keep))


def final_kernel(*refs, count, width):
    slots = [refs[7 * i : 7 * (i + 1)] for i in range(count)]
    start, rows_in, tap, *outs, out, conv, gates, local, lead, step, added, kept, conv_rows, y = refs[
        7 * count :
    ]
    z = here()[0]
    half = LANES // 2
    first, second, _, _, same = masks()
    mean_mat = jnp.where(same, 1.0 / half, 0.0).astype(BF)
    length = conv.shape[1]
    total_rows = count * length
    for at, slot in enumerate(slots):
        position = z ^ at
        for target, source in zip((conv, gates, local, lead, step, added, kept), slot):
            target[position] = source[...]

    middle = total_rows // 2
    pad = conv_rows.shape[0] - middle
    for block in range(count):
        pair = conv[block, :, :LANES].astype(F32)
        conv_in = (pair * pltpu.roll(sigmoid(pair), half, 1)).astype(BF).astype(F32)
        at = block * length
        if at < middle:
            conv_rows[pad + at : pad + at + length, :] = conv_in * first
            if at + length == middle:
                conv_rows[:pad, :] = pltpu.roll(conv_in[length - pad :, :], half, 1) * second
        else:
            rows = slice(pad + at - middle, pad + at - middle + length)
            conv_rows[rows, :] = conv_rows[rows, :] + pltpu.roll(conv_in, half, 1) * second
        out[at : at + length, LANES + half : 2 * LANES] = conv[block, :, LANES : LANES + half]
    tap = tap[:width, :]
    odd = (lax.rem(z, 2) == 1).astype(F32)
    left = iota((1, LANES), 1) < half
    tap = jnp.where(left == (odd < 0.5), tap, pltpu.roll(tap, half, 1))
    shift = pad - (width - 1)
    strip = 96
    for at in range(0, middle, strip):
        total = jnp.zeros((strip, LANES), F32)
        for j in range(width):
            total = total + tap[j : j + 1, :] * conv_rows[at + shift + j : at + shift + j + strip, :]
        total = total.astype(BF)
        out[at : at + strip, LANES : LANES + half] = total[:, :half]
        out[middle + at : middle + at + strip, LANES : LANES + half] = total[:, half:]

    state = start[...]
    chunks = length // SPAN
    for c in range(count * chunks):
        at = (c // chunks, c % chunks)
        low = state.astype(BF)
        seen = dot_nt(lead[at], low)
        y[c * SPAN : (c + 1) * SPAN, :] = local[at] + seen[:SPAN] + seen[SPAN:]
        state = state * kept[at][:1] + dot_nn(low, step[at]) + added[at]

    gain_row = rows_in[...]
    for block in range(count):
        rows = slice(block * length, (block + 1) * length)
        values = y[rows, :]
        high = values.astype(BF)
        low = (values - high.astype(F32)).astype(BF)
        centered = values - (dot_nn(high, mean_mat) + dot_nn(low, mean_mat))
        variance = dot_nn((centered * centered).astype(BF), mean_mat)
        gate = gates[block].astype(F32)
        grouped = centered * lax.rsqrt(variance + GROUP_FLOOR) * gain_row
        out[rows, :LANES] = (grouped * (gate * sigmoid(gate))).astype(BF)
    size = outs[0].shape[0]
    for at, target in enumerate(outs):
        row = ((z * lax.axis_size("tp") + here()[2]) ^ at) * size
        target[...] = out[pl.ds(pl.multiple_of(row, 32), size), :]


def output_kernel(point, *refs, groups):
    *operands, out, w, received = refs
    parts_in, pieces = operands[: received.shape[0]], operands[received.shape[0] :]
    z, f, t = here()
    count = pieces[0].shape[0]
    for at, part in enumerate(parts_in):
        received[(z * groups + t) ^ at] = part[...]
    split = count * LANES // 2
    wide = count * LANES
    gains = []
    for at, piece in enumerate(pieces):
        core, flip, side = at & 1, (at >> 1) & 1, (at >> 2) & 1
        group = t ^ side
        for block in range(count):
            col = pl.multiple_of((block * count + (f ^ (2 * flip) ^ core)) * LANES, LANES)
            for start, size, shift in (
                (0, split, group * split),
                (split, wide, groups * split + group * wide),
            ):
                w[pl.ds(pl.multiple_of(shift, LANES), size), pl.ds(col, LANES)] = piece[
                    block, start : start + size, :
                ]
        if core == flip == 0:
            spare = piece[0, split + wide :, :].astype(F32)
            tall = split // LANES
            parts = [spare[i * tall : (i + 1) * tall, :] for i in range(3)]
            total = parts[0] + parts[1] + parts[2]
            gains.append(jnp.concatenate([total[i : i + 1] for i in range(tall)], axis=1))
    gain = jnp.concatenate(
        [jnp.where(t == 0, gains[0], gains[1]), jnp.where(t == 0, gains[1], gains[0])], axis=1
    )
    half = LANES // 2
    sums, gates, states = [], [], []
    for group in range(groups):
        for block in range(count):
            source = received[block * groups + group]
            states.append(source[:, :LANES])
            sums.append(source[:, LANES : LANES + half])
            gates.append(source[:, LANES + half :])
    conv_sum = jnp.concatenate(sums, axis=1).astype(F32)
    gate = jnp.concatenate(gates, axis=1).astype(F32)
    mean = jnp.mean(conv_sum, axis=1, keepdims=True)
    spread = jnp.mean(conv_sum * conv_sum, axis=1, keepdims=True) - mean * mean
    scaled = (conv_sum - mean) * lax.rsqrt(spread + CHANNEL_FLOOR) * gain
    shaped = (scaled * sigmoid(scaled)).astype(BF)
    conv_out = (dot_nn(shaped, point[...]) * (gate * sigmoid(gate))).astype(BF)
    joined = jnp.concatenate([conv_out] + states, axis=1)
    out[...] = dot_nn(joined, w[...]).astype(BF)


def ordered_kernel(own, *refs):
    *sources, out = refs
    z = here()[0]
    out[z] = own[...]
    for step, choices in ARRIVALS:
        for at, holds in choices:

            def put(step=step, at=at):
                out[z ^ step] = sources[at][...]

            put() if holds is None else pl.when(holds(z))(put)


LINE = (
    ((0, 1), (1, 0), (2, 3), (3, 2)),
    ((0, 2), (1, 3), (2, 0), (3, 1)),
    ((1, 2), (2, 1)),
    ((2, 3), (1, 0)),
)
FORWARD = {3: 1}


def inner(z):
    return (z == 1) | (z == 2)


def outer(z):
    return (z == 0) | (z == 3)


ARRIVALS = (
    (1, ((0, None),)),
    (2, ((1, None),)),
    (3, ((2, inner), (3, outer))),
)


def along_line(value):
    moved = []
    for i, pairs in enumerate(LINE):
        moved.append(lax.ppermute(moved[FORWARD[i]] if i in FORWARD else value, "sp", pairs))
    return moved


def across(value, pairs):
    targets = sorted({b for _, b in pairs})
    return lax.ppermute(
        value, ("sp", "tp"), [(2 * i + s, 2 * i + 1 - s) for i in targets for s in (0, 1)]
    )


def flipped(value, axis, bit):
    count = lax.axis_size(axis)
    return lax.ppermute(value, axis, [(i, i ^ bit) for i in range(count)])


def head_body(
    tokens, decay_pace, start_state, norm_gain, conv_value, conv_admit, conv_gate, state_query,
    state_key, state_value, state_decay, state_gate, conv_taps, conv_gain, point_weight, decay_base,
    correction, group_gain, output_conv, output_state,
):
    width = tokens.shape[-1]
    length = tokens.shape[1]
    count, halves = lax.axis_size("sp"), lax.axis_size("tp")
    part = length // halves
    shard = conv_value.shape[0]
    columns = 7 * LANES
    slices = call(
        split_weights_kernel, [((shard, columns), BF)] * count,
        decay_pace, conv_value, conv_admit, conv_gate, state_query, state_key, state_value, state_decay,
        state_gate, held=range(9),
    )
    taken = [slices[0]] + [flipped(slices[k], "sp", k) for k in range(1, count)]
    out_rows = output_conv.shape[0] + output_state.shape[0]
    (rows_out,) = call(
        rows_kernel, [((out_rows + SPARE, output_conv.shape[1]), BF)],
        output_conv, output_state, conv_gain.reshape(1, -1), held=range(3),
    )
    normed, half = call(
        norm_kernel, [pltpu.HBM((length, width), BF), ((part, width), BF)],
        tokens.reshape(length, width), norm_gain.reshape(1, width), held=range(2),
    )
    line_out = along_line(rows_out)
    near = along_line(half)
    far = [across(a, LINE[i]) for i, a in enumerate(near)]
    lifted = [flipped(a, "fs", 2) for a in taken]
    (mine,) = call(assemble_kernel, [((2 * count * shard, columns), BF)], *taken, *lifted)
    sibling = flipped(mine, "fs", 1)
    (ordered,) = call(ordered_kernel, [((count,) + rows_out.shape, BF)], rows_out, *line_out)
    crossed = flipped(ordered, "tp", 1)
    pieces = []
    for a in (ordered, crossed):
        for b in (a, flipped(a, "fs", 2)):
            pieces += [b, flipped(b, "fs", 1)]
    total = length * count
    rows = total // (count * halves)
    chunks = length // SPAN
    terms = [
        ((length, 2 * LANES), BF),
        ((length, LANES), BF),
        ((chunks, SPAN, LANES), F32),
        ((chunks, LANES, LANES), BF),
        ((chunks, LANES, LANES), BF),
        ((chunks, LANES, LANES), F32),
        ((chunks, 8, LANES), F32),
    ]
    work = [((length, columns), F32), ((length, LANES), F32)]
    heads = start_state.shape[1]
    kernel = conv_taps.shape[0]
    begin, *small, gains, tap = call(
        prepare_kernel,
        [((LANES, LANES), F32)] + [((1, LANES), F32)] * 3 + [((-(-kernel // 8) * 8, LANES), F32)],
        start_state.reshape(heads, *start_state.shape[2:]), decay_base.reshape(1, -1),
        correction.reshape(1, -1), group_gain.reshape(1, -1), conv_taps, held=range(5),
    )
    w, *slots = call(
        own_kernel, [((width, columns), BF)] + terms,
        normed, mine, sibling, *small, held=(0,), scratch=work,
    )
    for step, choices in ARRIVALS:
        sources = [a for i, _ in choices for a in (near[i], far[i])]
        slots += call(
            block_kernel, terms, *sources, w, *small,
            scratch=work + [((length, width), BF)],
            step=step, conditions=tuple(holds for _, holds in choices),
        )
    mixed = call(
        final_kernel, [((rows, 2 * LANES), BF)] * (count * halves), *slots, begin, gains, tap,
        count=count, width=kernel,
        scratch=[((total, 2 * LANES), BF)]
        + [((count,) + a, b) for a, b in terms]
        + [((total // 2 + 32, LANES), F32), ((total, LANES), F32)],
    )
    received = [mixed[0]]
    for i in range(1, count * halves):
        received.append(
            lax.ppermute(mixed[i], ("sp", "tp"), [(d, d ^ i) for d in range(count * halves)])
        )
    (out,) = call(
        output_kernel, [jax.ShapeDtypeStruct((rows, width), BF)],
        point_weight, *received, *pieces, room=20, groups=halves,
        scratch=[((halves * out_rows, width), BF), ((count * halves, rows, 2 * LANES), BF)],
    )
    return out.reshape(1, rows, width)


def passed_along(value, axis, steps):
    count = lax.axis_size(axis)
    leading, last = (max(0, -steps), min(count, count - steps))
    return lax.ppermute(value, axis, [(source, source + steps) for source in range(leading, last)])


def entering_2(value, axis, join, neutral):
    place = lax.axis_index(axis)
    gathered = jax.tree.map(
        lambda a, kind: lax.all_gather(a.astype(kind), axis),
        value,
        jax.tree.map(lambda a: jnp.bfloat16 if a.dtype == jnp.float32 else a.dtype, value),
    )
    state = jax.tree.map(lambda a, e: jnp.zeros_like(a) + jnp.asarray(e, a.dtype), value, neutral)

    def one(lap, state):
        return join(
            state,
            jax.tree.map(
                lambda a, own: lax.dynamic_index_in_dim(a, lap, 0, False).astype(own.dtype),
                gathered,
                value,
            ),
        )

    return lax.fori_loop(0, place, one, state)


def apply_map(matrix, right):
    return jnp.einsum("hbti,hbic->hbtc", matrix, right, precision=lax.Precision.HIGHEST)


def pair_terms(left, right, mask):
    return jnp.einsum("hbtc,hbic->hbti", left, right, precision=lax.Precision.HIGHEST) * mask


def compose(earlier, later):
    first = jnp.matmul(earlier[0], later[0], precision=lax.Precision.HIGHEST)
    second = jnp.matmul(earlier[1], later[0], precision=lax.Precision.HIGHEST) + later[1]
    return (first, second)


def block_terms(query, keys, values, unit, write, log_keep):
    size = query.shape[-1]
    span = query.shape[2]
    total_log = jnp.cumsum(log_keep, axis=2)
    before_log = total_log - log_keep
    last_log = total_log[:, :, span - 1 :, :]
    lead_remove = -unit * jnp.exp(before_log)
    lead_query = query * jnp.exp(total_log)
    back_write = write * jnp.exp(-total_log)
    back_key = keys * jnp.exp(-total_log)
    places = jnp.arange(span)
    strict = (places[:, None] > places[None, :]).astype(jnp.float32)
    weak = (places[:, None] >= places[None, :]).astype(jnp.float32)
    remove_write = pair_terms(lead_remove, back_write, strict)
    remove_key = pair_terms(lead_remove, back_key, strict)
    query_write = pair_terms(lead_query, back_write, weak)
    query_key = pair_terms(lead_query, back_key, weak)
    right_side = jnp.concatenate([apply_map(remove_key, values), lead_remove], axis=-1)
    system = jnp.eye(span, dtype=jnp.float32) - remove_write
    solved = jax.scipy.linalg.solve_triangular(system, right_side, lower=True, unit_diagonal=True)
    own_part = solved[..., :size]
    start_part = solved[..., size:]
    local_out = apply_map(query_write, own_part) + apply_map(query_key, values)
    start_map = lead_query + apply_map(query_write, start_part)
    tail_write = write * jnp.exp(last_log - total_log)
    tail_key = keys * jnp.exp(last_log - total_log)
    carry_map = jnp.einsum(
        "hbtk,hbtj->hbkj", start_part, tail_write, precision=lax.Precision.HIGHEST
    ) + jnp.eye(size, dtype=jnp.float32) * jnp.exp(last_log)
    carry_add = jnp.einsum(
        "hbtv,hbtj->hbvj", own_part, tail_write, precision=lax.Precision.HIGHEST
    ) + jnp.einsum("hbtv,hbtj->hbvj", values, tail_key, precision=lax.Precision.HIGHEST)
    return (local_out, start_map, carry_map, carry_add)


def body(
    tokens,
    decay_pace,
    start_state,
    norm_gain,
    conv_value,
    conv_admit,
    conv_gate,
    state_query,
    state_key,
    state_value,
    state_decay,
    state_gate,
    conv_taps,
    conv_gain,
    point_weight,
    decay_base,
    correction,
    group_gain,
    output_conv,
    output_state,
):
    width = tokens.shape[-1]
    rows = tokens.reshape(-1, width)
    length = rows.shape[0]
    floats = rows.astype(jnp.float32)
    inverse = lax.rsqrt(jnp.mean(floats * floats, axis=1, keepdims=True) + NORM_FLOOR)
    normed = (floats * inverse * norm_gain).astype(jnp.bfloat16)
    shards = (
        conv_value,
        conv_admit,
        conv_gate,
        state_query,
        state_key,
        state_value,
        state_decay,
        state_gate,
    )
    stacked = jnp.concatenate(shards, axis=1)
    projected = jnp.dot(
        normed,
        lax.all_gather(stacked, ("sp", "fs"), axis=0, tiled=True),
        preferred_element_type=jnp.float32,
    ).astype(jnp.bfloat16)
    pieces = []
    offset = 0
    for shard in shards:
        pieces.append(projected[:, offset : offset + shard.shape[1]].astype(jnp.float32))
        offset = offset + shard.shape[1]
    value, admit, gate_conv, query, keys, values, decay_in, gate_state = pieces
    channels = value.shape[1]
    kernel = conv_taps.shape[0]
    conv_input = (value * jax.nn.sigmoid(admit)).astype(jnp.bfloat16)
    earlier = passed_along(conv_input[length - (kernel - 1) :], "sp", 1)
    padded = jnp.concatenate([earlier, conv_input], axis=0).astype(jnp.float32)
    conv_sum = jnp.zeros((length, channels), jnp.float32)
    for place in range(kernel):
        conv_sum = conv_sum + conv_taps[place] * padded[place : place + length]
    local_point = lax.dynamic_slice_in_dim(
        point_weight, lax.axis_index("tp") * channels, channels, 1
    )
    whole_sum, whole_gain = (
        lax.all_gather(conv_sum.astype(jnp.bfloat16), "tp", axis=1, tiled=True).astype(
            conv_sum.dtype
        ),
        lax.all_gather(conv_gain.astype(jnp.bfloat16), "tp", axis=0, tiled=True).astype(
            conv_gain.dtype
        ),
    )
    mean = jnp.mean(whole_sum, axis=1, keepdims=True)
    spread = jnp.mean(whole_sum * whole_sum, axis=1, keepdims=True) - mean * mean
    shaped = jax.nn.silu(
        (whole_sum - mean) * lax.rsqrt(spread + CHANNEL_FLOOR) * whole_gain
    ).astype(jnp.bfloat16)
    pointwise = jnp.dot(shaped, local_point, preferred_element_type=jnp.float32)
    conv_out = (pointwise * jax.nn.silu(gate_conv)).astype(jnp.bfloat16)
    size = start_state.shape[-1]
    heads = query.shape[1] // size
    span = min(64, length)
    blocks = length // span
    log_keep = -jnp.exp(decay_base + jnp.tanh(decay_in)) * decay_pace.reshape(-1)[:, None]
    key_heads = keys.reshape(length, heads, size)
    unit = key_heads * lax.rsqrt(
        jnp.maximum(jnp.sum(key_heads * key_heads, axis=-1, keepdims=True), 1.0)
    )
    write = unit * correction.reshape(heads, size)

    def arrange(array):
        return array.reshape(blocks, span, heads, size).transpose(2, 0, 1, 3)

    local_out, start_map, carry_map, carry_add = block_terms(
        arrange(query),
        arrange(keys),
        arrange(values),
        arrange(unit),
        arrange(write),
        arrange(log_keep),
    )
    identity = (
        jnp.broadcast_to(jnp.eye(size, dtype=jnp.float32), (heads, size, size)),
        jnp.zeros((heads, size, size), jnp.float32),
    )

    def along(carried, block_pair):
        return (compose(carried, block_pair), carried)

    device_pair, prefixes = lax.scan(
        along, identity, (jnp.moveaxis(carry_map, 1, 0), jnp.moveaxis(carry_add, 1, 0))
    )
    prior_map, prior_add = entering_2(device_pair, "sp", compose, identity)
    begin = start_state.reshape(heads, size, size)
    entering = jnp.matmul(begin, prior_map, precision=lax.Precision.HIGHEST) + prior_add
    block_starts = (
        jnp.matmul(entering[None], prefixes[0], precision=lax.Precision.HIGHEST) + prefixes[1]
    )
    block_starts = jnp.moveaxis(block_starts, 0, 1)
    outputs = local_out + jnp.einsum(
        "hbtk,hbvk->hbtv", start_map, block_starts, precision=lax.Precision.HIGHEST
    )
    outputs = outputs.transpose(1, 2, 0, 3).reshape(length, heads, size)
    centered = outputs - jnp.mean(outputs, axis=-1, keepdims=True)
    variance = jnp.mean(centered * centered, axis=-1, keepdims=True)
    grouped = centered * lax.rsqrt(variance + GROUP_FLOOR) * group_gain.reshape(heads, size)
    state_out = (grouped.reshape(length, heads * size) * jax.nn.silu(gate_state)).astype(
        jnp.bfloat16
    )
    local_mix = jnp.concatenate([conv_out, state_out], axis=1)
    moved = lax.all_to_all(local_mix, "tp", split_axis=0, concat_axis=1, tiled=True)
    conv_rows, state_rows = (
        lax.all_gather(output_conv, "tp", axis=0, tiled=True),
        lax.all_gather(output_state, "tp", axis=0, tiled=True),
    )
    groups = lax.axis_size("tp")
    joined = jnp.concatenate(
        [conv_rows.reshape(groups, channels, -1), state_rows.reshape(groups, heads * size, -1)],
        axis=1,
    )
    joined = joined.reshape(groups * (channels + heads * size), -1)
    mixed = jnp.dot(
        moved,
        lax.all_gather(joined, ("sp", "fs"), axis=1, tiled=True),
        preferred_element_type=jnp.float32,
    )
    return mixed.astype(jnp.bfloat16).reshape(1, -1, width)


def layer(*args):
    sizes = [lax.axis_size(a) for a in ("sp", "fs", "tp")]
    channels, wide = args[4].shape[1], args[7].shape[1]
    whole = channels == sizes[0] * LANES // 2 and wide == sizes[0] * LANES
    square = args[2].shape[-1] == LANES // 2 and args[4].shape[0] == LANES
    return (head_body if sizes == [4, 4, 2] and whole and square else body)(*args)


def solution(mesh):
    return jax.shard_map(
        layer,
        mesh=mesh,
        in_specs=(
            P("fs", "sp", None),
            P("fs", "sp"),
            P("fs", "tp", None, None),
            P(),
            P(("sp", "fs"), "tp"),
            P(("sp", "fs"), "tp"),
            P(("sp", "fs"), "tp"),
            P(("sp", "fs"), "tp"),
            P(("sp", "fs"), "tp"),
            P(("sp", "fs"), "tp"),
            P(("sp", "fs"), "tp"),
            P(("sp", "fs"), "tp"),
            P(None, "tp"),
            P("tp"),
            P(),
            P("tp"),
            P("tp"),
            P("tp"),
            P("tp", ("sp", "fs")),
            P("tp", ("sp", "fs")),
        ),
        out_specs=P("fs", ("sp", "tp"), None),
        check_vma=False,
    )
```
